512 devices in a mesh: sp: 64 (over z, y), tp: 8 (over x, core).
Axes of the slice: x: 4, y: 4, z: 16, core: 2. Of those that a mesh axis runs over, the one named last changes fastest.
Arguments:
- queries: bfloat16 [24576, 2048], P('sp', 'tp'), may hold values from -6 to 6
- key_heads: bfloat16 [24576, 1024], P('sp', 'tp'), may hold values from -6 to 6
- value_heads: bfloat16 [24576, 1024], P('sp', 'tp'), may hold values from -6 to 6
- sink_logit: float32 [16], P('tp'), may hold values from 3 to 7
- doc_ids: int32 [24576], replicated, may hold values from 0 to 15, never falling along the last dimension, each value on 1 to 3072 neighbouring positions
- residual: bfloat16 [24576, 2048], P('sp'), may hold values from -6 to 6
- out_proj: bfloat16 [2048, 2048], P('tp'), may hold values from -0.125 to 0.125
- gain_mix: float32 [2048], replicated, may hold values from 0.1 to 1.9
- up_proj: bfloat16 [2048, 8192], P('sp', 'tp'), may hold values from -0.125 to 0.125
- down_proj: bfloat16 [8192, 2048], P('tp', 'sp'), may hold values from -0.0625 to 0.0625
- gain_ffn_in: float32 [2048], replicated, may hold values from 0.1 to 1.9
- gain_ffn_out: float32 [2048], replicated, may hold values from 0.1 to 1.9
Outputs:
- layer_out: bfloat16 [24576, 2048], P(('sp', 'tp'))
The draws below stay inside these ranges and needn't reach their ends.
All inputs are finite; a program needn't handle non-finite values.
Results may differ from the reference program's by a relative error of at most 0.019.
Values may be sent and summed in bfloat16 or wider, within the bound.
No kernel may reach another device: no remote copies, remote signals or barrier semaphores. Data moves between devices by JAX's collectives and lax.ppermute only.
A program may use at most 64 MiB of HBM per device.

```python
import math
import jax
import jax.numpy as jnp
import numpy as np
from jax import lax

D = 2048
HEADS = 16
KV = 8
HD = 128
FF = 8192
WINDOW = 128
TOKENS = 24576
DOCS = 16
DOC_MOST = 3072
N_TP = 8


def draw_key_heads(key, part):
    noise_key = jax.random.fold_in(key, 2)
    noise = jax.random.normal(noise_key, (TOKENS, KV * HD), jnp.float32)
    return jnp.clip(noise, -6.0, 6.0).astype(jnp.bfloat16)


def draw_queries(key, part):
    noise_key = jax.random.fold_in(key, 1)
    noise = jax.random.normal(noise_key, (TOKENS, HEADS * HD), jnp.float32)
    return jnp.clip(noise, -6.0, 6.0).astype(jnp.bfloat16)


def level_of(key, extent, pieces, low, largest):
    loudness, own = 1.0, jax.random.fold_in(key, 6)
    for axis_at, shards_of in pieces:
        heights = jnp.exp(jax.random.uniform(jax.random.fold_in(own, axis_at), (shards_of,), jnp.float32, low / len(pieces), largest / len(pieces)))
        loudness = loudness * jnp.repeat(heights, extent[axis_at] // shards_of).reshape([-1 if axis == axis_at else 1 for axis in range(len(extent))])
    return loudness


def length_profile(amount, total, bound, slope):
    loads = [(1 << 20) // math.isqrt(rank ** slope) + 1 for rank in range(2, amount + 1)]
    spare, holding = total - bound - (amount - 1), [1] * (amount - 1)
    while spare > 0:
        movable = [i for i in range(amount - 1) if holding[i] < bound]
        mass, budget = sum([loads[i] for i in movable]), spare
        for i in movable:
            extra = min(bound - holding[i], max(1, budget * loads[i] // mass), spare)
            holding[i] = holding[i] + extra
            spare = spare - extra
    return np.array([bound] + holding)


def uneven_parts(own_key, amount, total, most, skew):
    if amount == 2:
        one = jax.random.randint(own_key, (), max(1, total - most), min(most, total - 1) + 1)
        return jnp.stack([one, total - one])
    sizes = jnp.asarray(length_profile(amount, total, most, skew), jnp.int32)
    couples = (amount - 1) // 2
    donor, sink = sizes[1:1 + 2 * couples:2], sizes[2:2 + 2 * couples:2]
    room = jnp.minimum(donor - 1, most - sink)
    shifted = jax.random.randint(jax.random.fold_in(own_key, 1), (couples,), 0, 1 << 20) % (room + 1)
    sizes = sizes.at[1:1 + 2 * couples:2].set(donor - shifted).at[2:2 + 2 * couples:2].set(sink + shifted)
    return sizes[jax.random.permutation(jax.random.fold_in(own_key, 2), amount)]


def centred(rng, dims, spread, bound, cuts=(), held_as=jnp.bfloat16):
    array = spread * jax.random.normal(rng, dims, jnp.float32)
    if cuts:
        array = array * level_of(rng, dims, cuts, -0.22, 0.18)
    return jnp.clip(array, -bound, bound).astype(held_as)


def setup_inputs(seed: int = 0) -> dict:
    keys = jax.random.split(jax.random.key(seed), 13)
    return {
        "queries": draw_queries(jax.random.fold_in(keys[12], 71), 0),
        "key_heads": draw_key_heads(jax.random.fold_in(keys[12], 71), 0),
        "value_heads": centred(keys[2], (TOKENS, KV * HD), 1.0, 6.0, ((0, 64), (1, 8))),
        "sink_logit": jnp.clip(3.0 + 4.0 * jax.random.uniform(keys[3], (HEADS,), jnp.float32) ** level_of(keys[3], (HEADS,), ((0, 8),), -0.2, 0.2), 3.0, 7.0),
        "doc_ids": jnp.searchsorted(jnp.cumsum(uneven_parts(keys[4], DOCS, TOKENS, DOC_MOST, 1)), jnp.arange(TOKENS), side="right").astype(jnp.int32),
        "residual": centred(keys[5], (TOKENS, D), 1.0, 6.0, ((0, 64),)),
        "out_proj": centred(keys[6], (HEADS * HD, D), (HEADS * HD) ** -0.5, 0.125, ((0, 8),)),
        "gain_mix": jnp.clip(1.0 + 0.18 * jax.random.normal(keys[7], (D,), jnp.float32), 0.1, 1.9),
        "up_proj": centred(keys[8], (D, FF), D ** -0.5, 0.125, ((0, 64), (1, 8))),
        "down_proj": centred(keys[9], (FF, D), FF ** -0.5, 0.0625, ((0, 8), (1, 64))),
        "gain_ffn_in": jnp.clip(1.0 + 0.18 * jax.random.normal(keys[10], (D,), jnp.float32), 0.1, 1.9),
        "gain_ffn_out": jnp.clip(1.0 + 0.18 * jax.random.normal(keys[11], (D,), jnp.float32), 0.1, 1.9),
    }


def rotate(field, places):
    half_dim = HD // 2
    inv_freq = 10000.0 ** (-jnp.arange(0, HD, 2, dtype=jnp.float32) / HD)
    angles = places[:, None, None] * inv_freq[None, None, :]
    cosine = jnp.cos(angles)
    sine = jnp.sin(angles)
    lower = field[..., :half_dim].astype(jnp.float32)
    upper = field[..., half_dim:].astype(jnp.float32)
    return jnp.concatenate([lower * cosine - upper * sine, upper * cosine + lower * sine], axis=-1).astype(jnp.bfloat16)

def banded(field, blocks):
    framed = field.reshape((blocks + 2, WINDOW) + field.shape[1:])
    return jnp.concatenate([framed[:-2], framed[1:-1], framed[2:]], axis=1)

def rms_scale(field, gain_vec):
    return field * lax.rsqrt(lax.optimization_barrier(jnp.mean(field * field, axis=-1, keepdims=True)) + 1e-06) * gain_vec

def reference(queries, key_heads, value_heads, sink_logit, doc_ids, residual, out_proj, gain_mix, up_proj, down_proj, gain_ffn_in, gain_ffn_out):
    length = queries.shape[0]
    blocks = length // WINDOW
    group_size = HEADS // KV
    places = jnp.arange(length).astype(jnp.float32)
    rotated_q = rotate(queries.reshape(length, HEADS, HD), places).reshape(blocks, WINDOW, KV, group_size, HD)
    rotated_k = rotate(key_heads.reshape(length, KV, HD), places)
    framing = ((WINDOW, WINDOW), (0, 0), (0, 0))
    key_win = banded(jnp.pad(rotated_k, framing), blocks)
    val_win = banded(jnp.pad(value_heads.reshape(length, KV, HD), framing), blocks)
    key_docs = banded(jnp.pad(doc_ids, (WINDOW, WINDOW), constant_values=-1), blocks)
    query_docs = doc_ids.reshape(blocks, WINDOW)
    q_index = jnp.arange(WINDOW)[:, None]
    k_index = jnp.arange(3 * WINDOW)[None, :]
    in_window = jnp.abs(k_index - WINDOW - q_index) <= WINDOW
    allowed = in_window[None] & (query_docs[:, :, None] == key_docs[:, None, :])

    def one_head(items):
        q_head, k_head, v_head, sink_vec = items
        scores = jnp.einsum('nqgd,nsd->ngqs', q_head.astype(jnp.float32), k_head.astype(jnp.float32)) * HD ** (-0.5)
        masked = jnp.where(allowed[:, None], scores, -1e+30)
        sink_col = sink_vec[None, :, None]
        top_score = jnp.maximum(lax.optimization_barrier(jnp.max(masked, axis=-1)), sink_col)
        exp_scores = jnp.where(allowed[:, None], jnp.exp(masked - top_score[..., None]), 0.0)
        denom_sum = lax.optimization_barrier(jnp.sum(exp_scores, axis=-1)) + jnp.exp(sink_col - top_score)
        probs = (exp_scores / denom_sum[..., None]).astype(jnp.bfloat16)
        return jnp.einsum('ngqs,nsd->nqgd', probs.astype(jnp.float32), v_head.astype(jnp.float32)).astype(jnp.bfloat16)
    attended = lax.map(one_head, (jnp.moveaxis(rotated_q, 2, 0), jnp.moveaxis(key_win, 2, 0), jnp.moveaxis(val_win, 2, 0), sink_logit.reshape(KV, group_size)))
    attn = jnp.moveaxis(attended, 0, 2).reshape(length, HEADS * HD)
    attn_cols = HEADS * HD // N_TP
    mixed = jnp.zeros((length, D), jnp.float32)
    for group in range(N_TP):
        partial_value = jnp.dot(attn[:, group * attn_cols:(group + 1) * attn_cols], out_proj[group * attn_cols:(group + 1) * attn_cols], preferred_element_type=jnp.float32).astype(jnp.bfloat16)
        mixed = mixed + lax.optimization_barrier(partial_value).astype(jnp.float32)
    after_mix = (residual.astype(jnp.float32) + rms_scale(mixed, gain_mix)).astype(jnp.bfloat16)
    normed = rms_scale(after_mix.astype(jnp.float32), gain_ffn_in).astype(jnp.bfloat16)
    hid_cols = FF // N_TP
    ffn_out = jnp.zeros((length, D), jnp.float32)
    for group in range(N_TP):
        up_acts = jnp.dot(normed, up_proj[:, group * hid_cols:(group + 1) * hid_cols], preferred_element_type=jnp.float32)
        hidden = jnp.square(jax.nn.relu(up_acts)).astype(jnp.bfloat16)
        partial_value = jnp.dot(hidden, down_proj[group * hid_cols:(group + 1) * hid_cols], preferred_element_type=jnp.float32).astype(jnp.bfloat16)
        ffn_out = ffn_out + lax.optimization_barrier(partial_value).astype(jnp.float32)
    return (after_mix.astype(jnp.float32) + rms_scale(ffn_out, gain_ffn_out)).astype(jnp.bfloat16)
```

```python
import jax
import jax.numpy as jnp
from jax import lax
from jax.sharding import PartitionSpec as P

HD = 128
WINDOW = 128


def fetch(shard, ahead, aside):
    pairs = [
        (4 * ((z + ahead) % 16) + (y + aside) % 4, 4 * z + y) for z in range(16) for y in range(4)
    ]
    return lax.ppermute(shard, "sp", pairs)


def placed(own, pieces, dim, own_at):
    whole = jnp.expand_dims(own, dim)
    whole = jnp.broadcast_to(whole, (*whole.shape[:dim], 4, *whole.shape[dim + 1 :]))
    for piece, away, cut, start in pieces:
        at = [0] * whole.ndim
        at[cut] = start
        at[dim] = (own_at + away) % 4
        whole = lax.dynamic_update_slice(whole, jnp.expand_dims(piece, dim), at)
    return whole


def far_stage(shard, far_at):
    pieces = [(fetch(shard, 4 * k, 0), k, 0, 0) for k in (1, 3, 2)]
    return placed(shard, pieces, 1, far_at)


def ring_stage(shard, along, dim, own_at, cut):
    def move(part, away):
        return fetch(part, away, 0) if along == "z" else fetch(part, 0, away)

    half = shard.shape[cut] // 2
    low = lax.slice_in_dim(shard, 0, half, axis=cut)
    high = lax.slice_in_dim(shard, half, 2 * half, axis=cut)
    whole_cut = cut + (dim <= cut)
    pieces = [(move(shard, 1), 1, 0, 0), (move(shard, -1), 3, 0, 0)]
    pieces += [(move(low, 2), 2, 0, 0), (move(high, -2), 2, whole_cut, half)]
    return placed(shard, pieces, dim, own_at)


def gathered_weights(up_proj, down_proj):
    place = lax.axis_index("sp")
    z, y = (place // 4, place % 4)
    both = jnp.stack([up_proj, down_proj.T])
    far = far_stage(both, z // 4)
    up = ring_stage(far[0], "y", 1, y, 0)
    down = ring_stage(far[1], "z", 1, z % 4, 0)
    up = ring_stage(up, "z", 1, z % 4, 0)
    down = ring_stage(down, "y", 2, y, 0)
    return up.reshape(2048, -1), down.reshape(2048, -1)


def padded(shard, sides, width):
    for axis, dim in sides:
        devices, length = (lax.axis_size(axis), shard.shape[dim])
        up = [(i, (i + 1) % devices) for i in range(devices - 1)]
        down = [(j, i) for i, j in up]
        last = lax.slice_in_dim(shard, length - width, length, axis=dim)
        first = lax.slice_in_dim(shard, 0, width, axis=dim)
        before = lax.ppermute(last, axis, up)
        after = lax.ppermute(first, axis, down)
        shard = jnp.concatenate([before, shard, after], axis=dim)
    return shard


def split_up(shard, dim, devices):
    before, after = (shard.shape[:dim], shard.shape[dim + 1 :])
    return jnp.moveaxis(shard.reshape(*before, devices, -1, *after), dim, 0)


def summed_on_arrival(shard, axis, dim):
    pieces = split_up(shard, dim, lax.axis_size(axis))
    arrived = lax.all_to_all(pieces, axis, split_axis=0, concat_axis=0, tiled=True)
    return arrived.astype(jnp.float32).sum(axis=0)


def joined_along(pieces, dim):
    pieces = jnp.moveaxis(pieces, 0, dim)
    lengths = pieces.shape
    return pieces.reshape(*lengths[:dim], lengths[dim] * lengths[dim + 1], *lengths[dim + 2 :])


def copy_for_each(shard, axis):
    devices = lax.axis_size(axis)
    return lax.all_to_all(
        jnp.broadcast_to(shard[None], (devices, *shard.shape)), axis, 0, 0, tiled=True
    )


def collect(shard, axis, dim):
    return joined_along(copy_for_each(shard, axis), dim)


def rotate(field, places):
    half_dim = HD // 2
    inv_freq = 10000.0 ** (-jnp.arange(0, HD, 2, dtype=jnp.float32) / HD)
    angles = places[:, None, None] * inv_freq[None, None, :]
    cosine = jnp.cos(angles)
    sine = jnp.sin(angles)
    lower = field[..., :half_dim].astype(jnp.float32)
    upper = field[..., half_dim:].astype(jnp.float32)
    return jnp.concatenate(
        [lower * cosine - upper * sine, upper * cosine + lower * sine], axis=-1
    ).astype(jnp.bfloat16)


def banded(field, blocks):
    framed = field.reshape((blocks + 2, WINDOW) + field.shape[1:])
    return jnp.concatenate([framed[:-2], framed[1:-1], framed[2:]], axis=1)


def rms_scale(field, gain_vec):
    return field * lax.rsqrt(jnp.mean(field * field, axis=-1, keepdims=True) + 1e-06) * gain_vec


def body(
    queries,
    key_heads,
    value_heads,
    sink_logit,
    doc_ids,
    residual,
    out_proj,
    gain_mix,
    up_proj,
    down_proj,
    gain_ffn_in,
    gain_ffn_out,
):
    tok_count = queries.shape[0]
    blocks = tok_count // WINDOW
    share_rows = tok_count // lax.axis_size("tp")
    q_local = queries.shape[1] // HD
    kv_local = key_heads.shape[1] // HD
    group_size = q_local // kv_local
    offset = lax.axis_index("sp") * tok_count
    up_whole, down_whole = gathered_weights(up_proj, down_proj)
    places = (offset + jnp.arange(tok_count)).astype(jnp.float32)
    rotated_q = rotate(queries.reshape(tok_count, q_local, HD), places).reshape(
        blocks, WINDOW, kv_local, group_size, HD
    )
    rotated_k = rotate(key_heads.reshape(tok_count, kv_local, HD), places).reshape(
        tok_count, kv_local * HD
    )
    rimmed = padded(jnp.stack([rotated_k, value_heads]), (("sp", 1),), WINDOW)
    key_win = banded(rimmed[0].reshape(-1, kv_local, HD), blocks)
    val_win = banded(rimmed[1].reshape(-1, kv_local, HD), blocks)
    padded_docs = jnp.pad(doc_ids, (WINDOW, WINDOW), constant_values=-1)
    key_docs = banded(lax.dynamic_slice_in_dim(padded_docs, offset, tok_count + 2 * WINDOW), blocks)
    query_docs = lax.dynamic_slice_in_dim(doc_ids, offset, tok_count).reshape(blocks, WINDOW)
    q_index = jnp.arange(WINDOW)[:, None]
    k_index = jnp.arange(3 * WINDOW)[None, :]
    in_window = jnp.abs(k_index - WINDOW - q_index) <= WINDOW
    allowed = (in_window[None] & (query_docs[:, :, None] == key_docs[:, None, :]))[:, None, None]
    scores = jnp.einsum(
        "nqkgd,nskd->nkgqs", rotated_q, key_win, preferred_element_type=jnp.float32
    ) * HD ** (-0.5)
    masked = jnp.where(allowed, scores, -1e30)
    sink_col = sink_logit.reshape(kv_local, group_size)[None, :, :, None]
    top_score = jnp.maximum(jnp.max(masked, axis=-1), sink_col)
    exp_scores = jnp.where(allowed, jnp.exp(masked - top_score[..., None]), 0.0)
    denom_sum = jnp.sum(exp_scores, axis=-1) + jnp.exp(sink_col - top_score)
    probs = (exp_scores / denom_sum[..., None]).astype(jnp.bfloat16)
    attn = (
        jnp.einsum("nkgqs,nskd->nqkgd", probs, val_win, preferred_element_type=jnp.float32)
        .astype(jnp.bfloat16)
        .reshape(tok_count, q_local * HD)
    )
    mixed = summed_on_arrival(
        jnp.dot(attn, out_proj, preferred_element_type=jnp.float32).astype(jnp.bfloat16), "tp", 0
    )
    own_resid = lax.dynamic_slice_in_dim(residual, lax.axis_index("tp") * share_rows, share_rows, 0)
    after_mix = (own_resid.astype(jnp.float32) + rms_scale(mixed, gain_mix)).astype(jnp.bfloat16)
    own_normed = rms_scale(after_mix.astype(jnp.float32), gain_ffn_in).astype(jnp.bfloat16)
    normed = collect(own_normed, "tp", 0)
    up_acts = jnp.dot(normed, up_whole, preferred_element_type=jnp.float32)
    hidden = jnp.square(jax.nn.relu(up_acts)).astype(jnp.bfloat16)
    ffn_out = summed_on_arrival(
        lax.dot_general(
            hidden, down_whole, (((1,), (1,)), ((), ())), preferred_element_type=jnp.float32
        ).astype(jnp.bfloat16),
        "tp",
        0,
    )
    return (after_mix.astype(jnp.float32) + rms_scale(ffn_out, gain_ffn_out)).astype(jnp.bfloat16)


def solution(mesh):
    return jax.shard_map(
        body,
        mesh=mesh,
        in_specs=(
            P("sp", "tp"),
            P("sp", "tp"),
            P("sp", "tp"),
            P("tp"),
            P(),
            P("sp", None),
            P("tp", None),
            P(),
            P("sp", "tp"),
            P("tp", "sp"),
            P(),
            P(),
        ),
        out_specs=P(("sp", "tp"), None),
        check_vma=False,
    )
```

```python
import jax
import jax.numpy as jnp
from jax import lax
from jax.sharding import PartitionSpec as P

HD = 128
WINDOW = 128


def fetch(shard, ahead, aside):
    pairs = [
        (4 * ((z + ahead) % 16) + (y + aside) % 4, 4 * z + y) for z in range(16) for y in range(4)
    ]
    return lax.ppermute(shard, "sp", pairs)


def placed(own, pieces, dim, own_at):
    whole = jnp.expand_dims(own, dim)
    whole = jnp.broadcast_to(whole, (*whole.shape[:dim], 4, *whole.shape[dim + 1 :]))
    for piece, away, cut, start in pieces:
        at = [0] * whole.ndim
        at[cut] = start
        at[dim] = (own_at + away) % 4
        whole = lax.dynamic_update_slice(whole, jnp.expand_dims(piece, dim), at)
    return whole


def far_stage(shard):
    rows = [(z % 4, y, 4 * z + y) for z in range(16) for y in range(4)]
    groups = [[i for a, b, i in rows if (a, b) == (c, d)] for c in range(4) for d in range(4)]
    spread = jnp.broadcast_to(shard[None], (4, *shard.shape))
    return lax.all_to_all(spread, "sp", 0, 0, axis_index_groups=groups, tiled=True)


def beside(shard, along):
    if along == "z":
        return fetch(shard, 1, 0), fetch(shard, -1, 0)
    return fetch(shard, 0, 1), fetch(shard, 0, -1)


def across_z(shard):
    half = shard.shape[0] // 2
    return fetch(shard[:half], 2, 0), fetch(shard[half:], -2, 0)


def joined_z(shard, near, far, dim, own_at):
    half = shard.shape[0] // 2
    pieces = [(near[0], 1, 0, 0), (near[1], 3, 0, 0)]
    pieces += [(far[0], 2, 0, 0), (far[1], 2, 0, half)]
    return placed(shard, pieces, dim, own_at)


def joined_y(shard, near, far, dim, own_at):
    pieces = [(near[0], 1, 0, 0), (near[1], 3, 0, 0), (far, 2, 0, 0)]
    return placed(shard, pieces, dim, own_at)


def start_weights(up_proj, down_proj):
    place = lax.axis_index("sp")
    z, y = (place // 4, place % 4)
    far = far_stage(jnp.stack([up_proj, down_proj.T]))
    up, down = (far[:, 0], far[:, 1])
    up = joined_y(up, beside(up, "y"), fetch(up, 0, 2), 1, y)
    down = joined_z(down, beside(down, "z"), across_z(down), 1, z % 4)
    return up, down, beside(up, "z"), beside(down, "y")


def finish_weights(up, down, up_near, down_near):
    place = lax.axis_index("sp")
    z, y = (place // 4, place % 4)
    up_far, down_far = (across_z(up), fetch(down, 0, 2))
    up_whole = joined_z(up, up_near, up_far, 1, z % 4)
    down_whole = joined_y(down, down_near, down_far, 2, y)
    return up_whole.reshape(2048, -1), down_whole.reshape(2048, -1)


def padded(shard, sides, width):
    for axis, dim in sides:
        devices, length = (lax.axis_size(axis), shard.shape[dim])
        up = [(i, (i + 1) % devices) for i in range(devices - 1)]
        down = [(j, i) for i, j in up]
        last = lax.slice_in_dim(shard, length - width, length, axis=dim)
        first = lax.slice_in_dim(shard, 0, width, axis=dim)
        before = lax.ppermute(last, axis, up)
        after = lax.ppermute(first, axis, down)
        shard = jnp.concatenate([before, shard, after], axis=dim)
    return shard


def split_up(shard, dim, devices):
    before, after = (shard.shape[:dim], shard.shape[dim + 1 :])
    return jnp.moveaxis(shard.reshape(*before, devices, -1, *after), dim, 0)


def summed_on_arrival(shard, axis, dim):
    pieces = split_up(shard, dim, lax.axis_size(axis))
    arrived = lax.all_to_all(pieces, axis, split_axis=0, concat_axis=0, tiled=True)
    return arrived.astype(jnp.float32).sum(axis=0)


def joined_along(pieces, dim):
    pieces = jnp.moveaxis(pieces, 0, dim)
    lengths = pieces.shape
    return pieces.reshape(*lengths[:dim], lengths[dim] * lengths[dim + 1], *lengths[dim + 2 :])


def copy_for_each(shard, axis):
    devices = lax.axis_size(axis)
    return lax.all_to_all(
        jnp.broadcast_to(shard[None], (devices, *shard.shape)), axis, 0, 0, tiled=True
    )


def collect(shard, axis, dim):
    return joined_along(copy_for_each(shard, axis), dim)


def rotate(field, places):
    half_dim = HD // 2
    inv_freq = 10000.0 ** (-jnp.arange(0, HD, 2, dtype=jnp.float32) / HD)
    angles = places[:, None, None] * inv_freq[None, None, :]
    cosine = jnp.cos(angles)
    sine = jnp.sin(angles)
    lower = field[..., :half_dim].astype(jnp.float32)
    upper = field[..., half_dim:].astype(jnp.float32)
    return jnp.concatenate(
        [lower * cosine - upper * sine, upper * cosine + lower * sine], axis=-1
    ).astype(jnp.bfloat16)


def banded(field, blocks):
    framed = field.reshape((blocks + 2, WINDOW) + field.shape[1:])
    return jnp.concatenate([framed[:-2], framed[1:-1], framed[2:]], axis=1)


def rms_scale(field, gain_vec):
    return field * lax.rsqrt(jnp.mean(field * field, axis=-1, keepdims=True) + 1e-06) * gain_vec


def body(
    queries,
    key_heads,
    value_heads,
    sink_logit,
    doc_ids,
    residual,
    out_proj,
    gain_mix,
    up_proj,
    down_proj,
    gain_ffn_in,
    gain_ffn_out,
):
    tok_count = queries.shape[0]
    blocks = tok_count // WINDOW
    share_rows = tok_count // lax.axis_size("tp")
    q_local = queries.shape[1] // HD
    kv_local = key_heads.shape[1] // HD
    group_size = q_local // kv_local
    offset = lax.axis_index("sp") * tok_count
    up, down, up_near, down_near = start_weights(up_proj, down_proj)
    places = (offset + jnp.arange(tok_count)).astype(jnp.float32)
    rotated_q = rotate(queries.reshape(tok_count, q_local, HD), places).reshape(
        blocks, WINDOW, kv_local, group_size, HD
    )
    rotated_k = rotate(key_heads.reshape(tok_count, kv_local, HD), places).reshape(
        tok_count, kv_local * HD
    )
    rimmed = padded(jnp.stack([rotated_k, value_heads]), (("sp", 1),), WINDOW)
    key_win = banded(rimmed[0].reshape(-1, kv_local, HD), blocks)
    val_win = banded(rimmed[1].reshape(-1, kv_local, HD), blocks)
    padded_docs = jnp.pad(doc_ids, (WINDOW, WINDOW), constant_values=-1)
    key_docs = banded(lax.dynamic_slice_in_dim(padded_docs, offset, tok_count + 2 * WINDOW), blocks)
    query_docs = lax.dynamic_slice_in_dim(doc_ids, offset, tok_count).reshape(blocks, WINDOW)
    q_index = jnp.arange(WINDOW)[:, None]
    k_index = jnp.arange(3 * WINDOW)[None, :]
    in_window = jnp.abs(k_index - WINDOW - q_index) <= WINDOW
    allowed = (in_window[None] & (query_docs[:, :, None] == key_docs[:, None, :]))[:, None, None]
    scores = jnp.einsum(
        "nqkgd,nskd->nkgqs", rotated_q, key_win, preferred_element_type=jnp.float32
    ) * HD ** (-0.5)
    masked = jnp.where(allowed, scores, -1e30)
    sink_col = sink_logit.reshape(kv_local, group_size)[None, :, :, None]
    top_score = jnp.maximum(jnp.max(masked, axis=-1), sink_col)
    exp_scores = jnp.where(allowed, jnp.exp(masked - top_score[..., None]), 0.0)
    denom_sum = jnp.sum(exp_scores, axis=-1) + jnp.exp(sink_col - top_score)
    probs = (exp_scores / denom_sum[..., None]).astype(jnp.bfloat16)
    attn = (
        jnp.einsum("nkgqs,nskd->nqkgd", probs, val_win, preferred_element_type=jnp.float32)
        .astype(jnp.bfloat16)
        .reshape(tok_count, q_local * HD)
    )
    partial_mix = jnp.dot(attn, out_proj, preferred_element_type=jnp.float32).astype(jnp.bfloat16)
    mixed = summed_on_arrival(partial_mix, "tp", 0)
    own_resid = lax.dynamic_slice_in_dim(residual, lax.axis_index("tp") * share_rows, share_rows, 0)
    after_mix = (own_resid.astype(jnp.float32) + rms_scale(mixed, gain_mix)).astype(jnp.bfloat16)
    own_normed = rms_scale(after_mix.astype(jnp.float32), gain_ffn_in).astype(jnp.bfloat16)
    up_whole, down_whole = finish_weights(up, down, up_near, down_near)
    normed = collect(own_normed, "tp", 0)
    up_acts = jnp.dot(normed, up_whole, preferred_element_type=jnp.float32)
    hidden = jnp.square(jax.nn.relu(up_acts)).astype(jnp.bfloat16)
    ffn_out = summed_on_arrival(
        lax.dot_general(
            hidden, down_whole, (((1,), (1,)), ((), ())), preferred_element_type=jnp.float32
        ).astype(jnp.bfloat16),
        "tp",
        0,
    )
    return (after_mix.astype(jnp.float32) + rms_scale(ffn_out, gain_ffn_out)).astype(jnp.bfloat16)


def solution(mesh):
    return jax.shard_map(
        body,
        mesh=mesh,
        in_specs=(
            P("sp", "tp"),
            P("sp", "tp"),
            P("sp", "tp"),
            P("tp"),
            P(),
            P("sp", None),
            P("tp", None),
            P(),
            P("sp", "tp"),
            P("tp", "sp"),
            P(),
            P(),
        ),
        out_specs=P(("sp", "tp"), None),
        check_vma=False,
    )
```

```python
import itertools

import jax
import jax.numpy as jnp
from jax import lax
from jax.sharding import PartitionSpec as P

HD = 128
WINDOW = 128


def fetch(shard, ahead, aside):
    pairs = [
        (4 * ((z + ahead) % 16) + (y + aside) % 4, 4 * z + y) for z in range(16) for y in range(4)
    ]
    return lax.ppermute(shard, "sp", pairs)


def placed(own, pieces, dim, own_at):
    whole = jnp.expand_dims(own, dim)
    whole = jnp.broadcast_to(whole, (*whole.shape[:dim], 4, *whole.shape[dim + 1 :]))
    for piece, away, cut, start in pieces:
        at = [0] * whole.ndim
        at[cut] = start
        at[dim] = (own_at + away) % 4
        whole = lax.dynamic_update_slice(whole, jnp.expand_dims(piece, dim), at)
    return whole


def far_stage(shard):
    rows = [(z % 4, y, 4 * z + y) for z in range(16) for y in range(4)]
    groups = [[i for a, b, i in rows if (a, b) == (c, d)] for c in range(4) for d in range(4)]
    spread = jnp.broadcast_to(shard[None], (4, *shard.shape))
    return lax.all_to_all(spread, "sp", 0, 0, axis_index_groups=groups, tiled=True)


def beside(shard, along):
    if along == "z":
        return fetch(shard, 1, 0), fetch(shard, -1, 0)
    return fetch(shard, 0, 1), fetch(shard, 0, -1)


def across_z(shard):
    half = shard.shape[0] // 2
    return fetch(shard[:half], 2, 0), fetch(shard[half:], -2, 0)


def joined_z(shard, near, far, dim, own_at):
    half = shard.shape[0] // 2
    pieces = [(near[0], 1, 0, 0), (near[1], 3, 0, 0)]
    pieces += [(far[0], 2, 0, 0), (far[1], 2, 0, half)]
    return placed(shard, pieces, dim, own_at)


def joined_y(shard, other, dim, own_at):
    whole = jnp.expand_dims(shard, dim)
    whole = jnp.broadcast_to(whole, (*whole.shape[:dim], 2, *whole.shape[dim + 1 :]))
    at = [0] * whole.ndim
    at[dim] = 1 - own_at
    return lax.dynamic_update_slice(whole, jnp.expand_dims(other, dim), at)


def device(z, y, x, core):
    return (4 * z + y) * 8 + 2 * x + core


def paired(shard):
    pairs = []
    for z, y, x, core in itertools.product(range(16), range(4), range(4), range(2)):
        own = device(z, y, x, core)
        pairs.append((own, own if core == y % 2 else device(z, y ^ 1, x, 1 - core)))
    return lax.ppermute(shard, ("sp", "tp"), pairs)


def swapped(shard):
    return lax.ppermute(shard, "tp", [(i, i ^ 1) for i in range(8)])


def token_groups():
    return [
        [device(z, 2 * q + par, x, core) for par in range(2) for x in range(4)]
        for z in range(16)
        for q in range(2)
        for core in range(2)
    ]


def exchanged(pieces):
    return lax.all_to_all(
        pieces, ("sp", "tp"), 0, 0, axis_index_groups=token_groups(), tiled=True
    )


def halves(field, core):
    first, second = (field[:, 0], field[:, 1])
    return jnp.where(core == 0, first, second), jnp.where(core == 0, second, first)


def start_weights(up_proj, down_proj):
    place = lax.axis_index("sp")
    z, y = (place // 4, place % 4)
    both = paired(jnp.stack([up_proj, down_proj.T]))
    far = far_stage(both)
    up, down = (far[:, 0], far[:, 1])
    up_other = fetch(up, 0, 2)
    down_near, down_far = (beside(down, "z"), across_z(down))
    up = joined_y(up, up_other, 1, y // 2)
    down = joined_z(down, down_near, down_far, 1, z % 4)
    up_near, up_far, down_other = (beside(up, "z"), across_z(up), fetch(down, 0, 2))
    up = joined_z(up, up_near, up_far, 1, z % 4).reshape(1024, 1024)
    down = joined_y(down, down_other, 2, y // 2).reshape(1024, 1024)
    return up, swapped(up), down, swapped(down)


def padded(shard, sides, width):
    for axis, dim in sides:
        devices, length = (lax.axis_size(axis), shard.shape[dim])
        up = [(i, (i + 1) % devices) for i in range(devices - 1)]
        down = [(j, i) for i, j in up]
        last = lax.slice_in_dim(shard, length - width, length, axis=dim)
        first = lax.slice_in_dim(shard, 0, width, axis=dim)
        before = lax.ppermute(last, axis, up)
        after = lax.ppermute(first, axis, down)
        shard = jnp.concatenate([before, shard, after], axis=dim)
    return shard


def split_up(shard, dim, devices):
    before, after = (shard.shape[:dim], shard.shape[dim + 1 :])
    return jnp.moveaxis(shard.reshape(*before, devices, -1, *after), dim, 0)


def summed_on_arrival(shard, axis, dim):
    pieces = split_up(shard, dim, lax.axis_size(axis))
    arrived = lax.all_to_all(pieces, axis, split_axis=0, concat_axis=0, tiled=True)
    return arrived.astype(jnp.float32).sum(axis=0)


def rotate(field, places):
    half_dim = HD // 2
    inv_freq = 10000.0 ** (-jnp.arange(0, HD, 2, dtype=jnp.float32) / HD)
    angles = places[:, None, None] * inv_freq[None, None, :]
    cosine = jnp.cos(angles)
    sine = jnp.sin(angles)
    lower = field[..., :half_dim].astype(jnp.float32)
    upper = field[..., half_dim:].astype(jnp.float32)
    return jnp.concatenate(
        [lower * cosine - upper * sine, upper * cosine + lower * sine], axis=-1
    ).astype(jnp.bfloat16)


def banded(field, blocks):
    framed = field.reshape((blocks + 2, WINDOW) + field.shape[1:])
    return jnp.concatenate([framed[:-2], framed[1:-1], framed[2:]], axis=1)


def rms_scale(field, gain_vec):
    return field * lax.rsqrt(jnp.mean(field * field, axis=-1, keepdims=True) + 1e-06) * gain_vec


def body(
    queries,
    key_heads,
    value_heads,
    sink_logit,
    doc_ids,
    residual,
    out_proj,
    gain_mix,
    up_proj,
    down_proj,
    gain_ffn_in,
    gain_ffn_out,
):
    tok_count = queries.shape[0]
    blocks = tok_count // WINDOW
    share_rows = tok_count // lax.axis_size("tp")
    q_local = queries.shape[1] // HD
    kv_local = key_heads.shape[1] // HD
    group_size = q_local // kv_local
    offset = lax.axis_index("sp") * tok_count
    up, up_other, down, down_other = start_weights(up_proj, down_proj)
    core = lax.axis_index("tp") % 2
    places = (offset + jnp.arange(tok_count)).astype(jnp.float32)
    rotated_q = rotate(queries.reshape(tok_count, q_local, HD), places).reshape(
        blocks, WINDOW, kv_local, group_size, HD
    )
    rotated_k = rotate(key_heads.reshape(tok_count, kv_local, HD), places).reshape(
        tok_count, kv_local * HD
    )
    rimmed = padded(jnp.stack([rotated_k, value_heads]), (("sp", 1),), WINDOW)
    key_win = banded(rimmed[0].reshape(-1, kv_local, HD), blocks)
    val_win = banded(rimmed[1].reshape(-1, kv_local, HD), blocks)
    padded_docs = jnp.pad(doc_ids, (WINDOW, WINDOW), constant_values=-1)
    key_docs = banded(lax.dynamic_slice_in_dim(padded_docs, offset, tok_count + 2 * WINDOW), blocks)
    query_docs = lax.dynamic_slice_in_dim(doc_ids, offset, tok_count).reshape(blocks, WINDOW)
    q_index = jnp.arange(WINDOW)[:, None]
    k_index = jnp.arange(3 * WINDOW)[None, :]
    in_window = jnp.abs(k_index - WINDOW - q_index) <= WINDOW
    allowed = (in_window[None] & (query_docs[:, :, None] == key_docs[:, None, :]))[:, None, None]
    scores = jnp.einsum(
        "nqkgd,nskd->nkgqs", rotated_q, key_win, preferred_element_type=jnp.float32
    ) * HD ** (-0.5)
    masked = jnp.where(allowed, scores, -1e30)
    sink_col = sink_logit.reshape(kv_local, group_size)[None, :, :, None]
    top_score = jnp.maximum(jnp.max(masked, axis=-1), sink_col)
    exp_scores = jnp.where(allowed, jnp.exp(masked - top_score[..., None]), 0.0)
    denom_sum = jnp.sum(exp_scores, axis=-1) + jnp.exp(sink_col - top_score)
    probs = (exp_scores / denom_sum[..., None]).astype(jnp.bfloat16)
    attn = (
        jnp.einsum("nkgqs,nskd->nqkgd", probs, val_win, preferred_element_type=jnp.float32)
        .astype(jnp.bfloat16)
        .reshape(tok_count, q_local * HD)
    )
    partial_mix = jnp.dot(attn, out_proj, preferred_element_type=jnp.float32).astype(jnp.bfloat16)
    mixed = summed_on_arrival(partial_mix, "tp", 0)
    own_resid = lax.dynamic_slice_in_dim(residual, lax.axis_index("tp") * share_rows, share_rows, 0)
    after_mix = (own_resid.astype(jnp.float32) + rms_scale(mixed, gain_mix)).astype(jnp.bfloat16)
    own_normed = rms_scale(after_mix.astype(jnp.float32), gain_ffn_in).astype(jnp.bfloat16)
    first, second = halves(own_normed.reshape(-1, 32, 2, 32).swapaxes(1, 2), core)
    ordered = jnp.concatenate([first.reshape(-1, 1024), second.reshape(-1, 1024)], axis=1)
    normed = exchanged(jnp.broadcast_to(ordered[None], (8, *ordered.shape)))
    normed = normed.reshape(-1, 2048)
    up_acts = jnp.dot(normed[:, :1024], up, preferred_element_type=jnp.float32) + jnp.dot(
        normed[:, 1024:], up_other, preferred_element_type=jnp.float32
    )
    hidden = jnp.square(jax.nn.relu(up_acts)).astype(jnp.bfloat16)
    across = (((1,), (1,)), ((), ()))
    parts = [
        lax.dot_general(hidden, w, across, preferred_element_type=jnp.float32).astype(jnp.bfloat16)
        for w in (down, down_other)
    ]
    arrived = exchanged(jnp.concatenate(parts, axis=1).reshape(8, -1, 2048))
    summed = arrived.astype(jnp.float32).sum(axis=0).reshape(-1, 2, 32, 32)
    ffn_out = jnp.stack(halves(summed, core), axis=2).reshape(-1, 2048)
    return (after_mix.astype(jnp.float32) + rms_scale(ffn_out, gain_ffn_out)).astype(jnp.bfloat16)


def solution(mesh):
    return jax.shard_map(
        body,
        mesh=mesh,
        in_specs=(
            P("sp", "tp"),
            P("sp", "tp"),
            P("sp", "tp"),
            P("tp"),
            P(),
            P("sp", None),
            P("tp", None),
            P(),
            P("sp", "tp"),
            P("tp", "sp"),
            P(),
            P(),
        ),
        out_specs=P(("sp", "tp"), None),
        check_vma=False,
    )
```

```python
import itertools

import jax
import jax.numpy as jnp
from jax import lax
from jax.sharding import PartitionSpec as P

HD = 128
WINDOW = 128


def fetch(shard, ahead, aside):
    pairs = [
        (4 * ((z + ahead) % 16) + (y + aside) % 4, 4 * z + y) for z in range(16) for y in range(4)
    ]
    return lax.ppermute(shard, "sp", pairs)


def placed(own, pieces, dim, own_at):
    whole = jnp.expand_dims(own, dim)
    whole = jnp.broadcast_to(whole, (*whole.shape[:dim], 4, *whole.shape[dim + 1 :]))
    for piece, away, cut, start in pieces:
        at = [0] * whole.ndim
        at[cut] = start
        at[dim] = (own_at + away) % 4
        whole = lax.dynamic_update_slice(whole, jnp.expand_dims(piece, dim), at)
    return whole


def far_stage(shard):
    rows = [(z % 4, y, 4 * z + y) for z in range(16) for y in range(4)]
    groups = [[i for a, b, i in rows if (a, b) == (c, d)] for c in range(4) for d in range(4)]
    spread = jnp.broadcast_to(shard[None], (4, *shard.shape))
    return lax.all_to_all(spread, "sp", 0, 0, axis_index_groups=groups, tiled=True)


def beside(shard, along):
    if along == "z":
        return fetch(shard, 1, 0), fetch(shard, -1, 0)
    return fetch(shard, 0, 1), fetch(shard, 0, -1)


def across_z(shard):
    half = shard.shape[0] // 2
    return fetch(shard[:half], 2, 0), fetch(shard[half:], -2, 0)


def joined_y(shard, other, dim, own_at):
    whole = jnp.expand_dims(shard, dim)
    whole = jnp.broadcast_to(whole, (*whole.shape[:dim], 2, *whole.shape[dim + 1 :]))
    at = [0] * whole.ndim
    at[dim] = 1 - own_at
    return lax.dynamic_update_slice(whole, jnp.expand_dims(other, dim), at)


def device(z, y, x, core):
    return (4 * z + y) * 8 + 2 * x + core


def paired(shard):
    pairs = []
    for z, y, x, core in itertools.product(range(16), range(4), range(4), range(2)):
        own = device(z, y, x, core)
        pairs.append((own, own if core == y % 2 else device(z, y ^ 1, x, 1 - core)))
    return lax.ppermute(shard, ("sp", "tp"), pairs)


def swapped(shard):
    return lax.ppermute(shard, "tp", [(i, i ^ 1) for i in range(8)])


def token_groups():
    return [
        [device(z, 2 * q + par, x, core) for par in range(2) for x in range(4)]
        for z in range(16)
        for q in range(2)
        for core in range(2)
    ]


def exchanged(pieces):
    return lax.all_to_all(
        pieces, ("sp", "tp"), 0, 0, axis_index_groups=token_groups(), tiled=True
    )


def halves(field, core):
    first, second = (field[:, 0], field[:, 1])
    return jnp.where(core == 0, first, second), jnp.where(core == 0, second, first)


def start_weights(up_proj, down_proj):
    place = lax.axis_index("sp")
    z, y = (place // 4, place % 4)
    both = paired(jnp.stack([up_proj, down_proj.T]))
    far = far_stage(both)
    both = far.swapaxes(0, 1)
    other = fetch(both, 0, 2)
    both = joined_y(both, other, 2, y // 2)
    near, across = (beside(both, "z"), across_z(both))
    up, down = (
        placed(
            both[i],
            [(near[0][i], 1, 0, 0), (near[1][i], 3, 0, 0), (across[i][0], 2, 0, 0)],
            1,
            z % 4,
        ).reshape(1024, 1024)
        for i in range(2)
    )
    return up, swapped(up), down, swapped(down)


def padded(shard, sides, width):
    for axis, dim in sides:
        devices, length = (lax.axis_size(axis), shard.shape[dim])
        up = [(i, (i + 1) % devices) for i in range(devices - 1)]
        down = [(j, i) for i, j in up]
        last = lax.slice_in_dim(shard, length - width, length, axis=dim)
        first = lax.slice_in_dim(shard, 0, width, axis=dim)
        before = lax.ppermute(last, axis, up)
        after = lax.ppermute(first, axis, down)
        shard = jnp.concatenate([before, shard, after], axis=dim)
    return shard


def split_up(shard, dim, devices):
    before, after = (shard.shape[:dim], shard.shape[dim + 1 :])
    return jnp.moveaxis(shard.reshape(*before, devices, -1, *after), dim, 0)


def summed_on_arrival(shard, axis, dim):
    pieces = split_up(shard, dim, lax.axis_size(axis))
    arrived = lax.all_to_all(pieces, axis, split_axis=0, concat_axis=0, tiled=True)
    return arrived.astype(jnp.float32).sum(axis=0)


def rotate(field, places):
    half_dim = HD // 2
    inv_freq = 10000.0 ** (-jnp.arange(0, HD, 2, dtype=jnp.float32) / HD)
    angles = places[:, None, None] * inv_freq[None, None, :]
    cosine = jnp.cos(angles)
    sine = jnp.sin(angles)
    lower = field[..., :half_dim].astype(jnp.float32)
    upper = field[..., half_dim:].astype(jnp.float32)
    return jnp.concatenate(
        [lower * cosine - upper * sine, upper * cosine + lower * sine], axis=-1
    ).astype(jnp.bfloat16)


def banded(field, blocks):
    framed = field.reshape((blocks + 2, WINDOW) + field.shape[1:])
    return jnp.concatenate([framed[:-2], framed[1:-1], framed[2:]], axis=1)


def rms_scale(field, gain_vec):
    return field * lax.rsqrt(jnp.mean(field * field, axis=-1, keepdims=True) + 1e-06) * gain_vec


def body(
    queries,
    key_heads,
    value_heads,
    sink_logit,
    doc_ids,
    residual,
    out_proj,
    gain_mix,
    up_proj,
    down_proj,
    gain_ffn_in,
    gain_ffn_out,
):
    tok_count = queries.shape[0]
    blocks = tok_count // WINDOW
    share_rows = tok_count // lax.axis_size("tp")
    q_local = queries.shape[1] // HD
    kv_local = key_heads.shape[1] // HD
    group_size = q_local // kv_local
    offset = lax.axis_index("sp") * tok_count
    up, up_other, down, down_other = start_weights(up_proj, down_proj)
    core = lax.axis_index("tp") % 2
    places = (offset + jnp.arange(tok_count)).astype(jnp.float32)
    rotated_q = rotate(queries.reshape(tok_count, q_local, HD), places).reshape(
        blocks, WINDOW, kv_local, group_size, HD
    )
    rotated_k = rotate(key_heads.reshape(tok_count, kv_local, HD), places).reshape(
        tok_count, kv_local * HD
    )
    rimmed = padded(jnp.stack([rotated_k, value_heads]), (("sp", 1),), WINDOW)
    key_win = banded(rimmed[0].reshape(-1, kv_local, HD), blocks)
    val_win = banded(rimmed[1].reshape(-1, kv_local, HD), blocks)
    padded_docs = jnp.pad(doc_ids, (WINDOW, WINDOW), constant_values=-1)
    key_docs = banded(lax.dynamic_slice_in_dim(padded_docs, offset, tok_count + 2 * WINDOW), blocks)
    query_docs = lax.dynamic_slice_in_dim(doc_ids, offset, tok_count).reshape(blocks, WINDOW)
    q_index = jnp.arange(WINDOW)[:, None]
    k_index = jnp.arange(3 * WINDOW)[None, :]
    in_window = jnp.abs(k_index - WINDOW - q_index) <= WINDOW
    allowed = (in_window[None] & (query_docs[:, :, None] == key_docs[:, None, :]))[:, None, None]
    scores = jnp.einsum(
        "nqkgd,nskd->nkgqs", rotated_q, key_win, preferred_element_type=jnp.float32
    ) * HD ** (-0.5)
    masked = jnp.where(allowed, scores, -1e30)
    sink_col = sink_logit.reshape(kv_local, group_size)[None, :, :, None]
    top_score = jnp.maximum(jnp.max(masked, axis=-1), sink_col)
    exp_scores = jnp.where(allowed, jnp.exp(masked - top_score[..., None]), 0.0)
    denom_sum = jnp.sum(exp_scores, axis=-1) + jnp.exp(sink_col - top_score)
    probs = (exp_scores / denom_sum[..., None]).astype(jnp.bfloat16)
    attn = (
        jnp.einsum("nkgqs,nskd->nqkgd", probs, val_win, preferred_element_type=jnp.float32)
        .astype(jnp.bfloat16)
        .reshape(tok_count, q_local * HD)
    )
    partial_mix = jnp.dot(attn, out_proj, preferred_element_type=jnp.float32).astype(jnp.bfloat16)
    mixed = summed_on_arrival(partial_mix, "tp", 0)
    own_resid = lax.dynamic_slice_in_dim(residual, lax.axis_index("tp") * share_rows, share_rows, 0)
    after_mix = (own_resid.astype(jnp.float32) + rms_scale(mixed, gain_mix)).astype(jnp.bfloat16)
    own_normed = rms_scale(after_mix.astype(jnp.float32), gain_ffn_in).astype(jnp.bfloat16)
    first, second = halves(own_normed.reshape(-1, 32, 2, 32).swapaxes(1, 2), core)
    ordered = jnp.concatenate([first.reshape(-1, 1024), second.reshape(-1, 1024)], axis=1)
    normed = exchanged(jnp.broadcast_to(ordered[None], (8, *ordered.shape)))
    normed = normed.reshape(-1, 2048)
    up_acts = jnp.dot(normed[:, :1024], up, preferred_element_type=jnp.float32) + jnp.dot(
        normed[:, 1024:], up_other, preferred_element_type=jnp.float32
    )
    hidden = jnp.square(jax.nn.relu(up_acts)).astype(jnp.bfloat16)
    across = (((1,), (1,)), ((), ()))
    parts = [
        lax.dot_general(hidden, w, across, preferred_element_type=jnp.float32).astype(jnp.bfloat16)
        for w in (down, down_other)
    ]
    arrived = exchanged(jnp.concatenate(parts, axis=1).reshape(8, -1, 2048))
    summed = arrived.astype(jnp.float32).sum(axis=0).reshape(-1, 2, 32, 32)
    ffn_out = jnp.stack(halves(summed, core), axis=2).reshape(-1, 2048)
    return (after_mix.astype(jnp.float32) + rms_scale(ffn_out, gain_ffn_out)).astype(jnp.bfloat16)


def solution(mesh):
    return jax.shard_map(
        body,
        mesh=mesh,
        in_specs=(
            P("sp", "tp"),
            P("sp", "tp"),
            P("sp", "tp"),
            P("tp"),
            P(),
            P("sp", None),
            P("tp", None),
            P(),
            P("sp", "tp"),
            P("tp", "sp"),
            P(),
            P(),
        ),
        out_specs=P(("sp", "tp"), None),
        check_vma=False,
    )
```

```python
import jax
import jax.numpy as jnp
from jax import lax
from jax.sharding import PartitionSpec as P

HD = 128
WINDOW = 128


def device(z, y, x, core):
    return (4 * z + y) * 8 + 2 * x + core


def group_weights(up_proj, down_proj):
    columns = [w.reshape(32, 4, 256).swapaxes(0, 1) for w in (up_proj, down_proj.T)]
    along_y = [[4 * z + y for y in range(4)] for z in range(16)]
    along_z = [[4 * z + y for z in range(16)] for y in range(4)]
    rows = lax.all_to_all(
        jnp.concatenate(columns, axis=2), "sp", 0, 0, axis_index_groups=along_y, tiled=True
    )
    own = lax.all_gather(
        rows.reshape(128, 512), "sp", axis=0, tiled=True, axis_index_groups=along_z
    )
    return own, lax.ppermute(own, "tp", [(i, i ^ 1) for i in range(8)])


def exchanged(pieces):
    groups = [
        [device(z, y, x, core) for y in range(4) for x in range(4)]
        for z in range(16)
        for core in range(2)
    ]
    return lax.all_to_all(pieces, ("sp", "tp"), 0, 0, axis_index_groups=groups, tiled=True)


def padded(shard, sides, width):
    for axis, dim in sides:
        devices, length = (lax.axis_size(axis), shard.shape[dim])
        up = [(i, (i + 1) % devices) for i in range(devices - 1)]
        down = [(j, i) for i, j in up]
        last = lax.slice_in_dim(shard, length - width, length, axis=dim)
        first = lax.slice_in_dim(shard, 0, width, axis=dim)
        before = lax.ppermute(last, axis, up)
        after = lax.ppermute(first, axis, down)
        shard = jnp.concatenate([before, shard, after], axis=dim)
    return shard


def split_up(shard, dim, devices):
    before, after = (shard.shape[:dim], shard.shape[dim + 1 :])
    return jnp.moveaxis(shard.reshape(*before, devices, -1, *after), dim, 0)


def summed_on_arrival(shard, axis, dim):
    pieces = split_up(shard, dim, lax.axis_size(axis))
    arrived = lax.all_to_all(pieces, axis, split_axis=0, concat_axis=0, tiled=True)
    return arrived.astype(jnp.float32).sum(axis=0)


def rotate(field, places):
    half_dim = HD // 2
    inv_freq = 10000.0 ** (-jnp.arange(0, HD, 2, dtype=jnp.float32) / HD)
    angles = places[:, None, None] * inv_freq[None, None, :]
    cosine = jnp.cos(angles)
    sine = jnp.sin(angles)
    lower = field[..., :half_dim].astype(jnp.float32)
    upper = field[..., half_dim:].astype(jnp.float32)
    return jnp.concatenate(
        [lower * cosine - upper * sine, upper * cosine + lower * sine], axis=-1
    ).astype(jnp.bfloat16)


def banded(field, blocks):
    framed = field.reshape((blocks + 2, WINDOW) + field.shape[1:])
    return jnp.concatenate([framed[:-2], framed[1:-1], framed[2:]], axis=1)


def rms_scale(field, gain_vec):
    return field * lax.rsqrt(jnp.mean(field * field, axis=-1, keepdims=True) + 1e-06) * gain_vec


def body(
    queries,
    key_heads,
    value_heads,
    sink_logit,
    doc_ids,
    residual,
    out_proj,
    gain_mix,
    up_proj,
    down_proj,
    gain_ffn_in,
    gain_ffn_out,
):
    tok_count = queries.shape[0]
    blocks = tok_count // WINDOW
    share_rows = tok_count // lax.axis_size("tp")
    q_local = queries.shape[1] // HD
    kv_local = key_heads.shape[1] // HD
    group_size = q_local // kv_local
    offset = lax.axis_index("sp") * tok_count
    weights = group_weights(up_proj, down_proj)
    places = (offset + jnp.arange(tok_count)).astype(jnp.float32)
    rotated_q = rotate(queries.reshape(tok_count, q_local, HD), places).reshape(
        blocks, WINDOW, kv_local, group_size, HD
    )
    rotated_k = rotate(key_heads.reshape(tok_count, kv_local, HD), places).reshape(
        tok_count, kv_local * HD
    )
    rimmed = padded(jnp.stack([rotated_k, value_heads]), (("sp", 1),), WINDOW)
    key_win = banded(rimmed[0].reshape(-1, kv_local, HD), blocks)
    val_win = banded(rimmed[1].reshape(-1, kv_local, HD), blocks)
    padded_docs = jnp.pad(doc_ids, (WINDOW, WINDOW), constant_values=-1)
    key_docs = banded(lax.dynamic_slice_in_dim(padded_docs, offset, tok_count + 2 * WINDOW), blocks)
    query_docs = lax.dynamic_slice_in_dim(doc_ids, offset, tok_count).reshape(blocks, WINDOW)
    q_index = jnp.arange(WINDOW)[:, None]
    k_index = jnp.arange(3 * WINDOW)[None, :]
    in_window = jnp.abs(k_index - WINDOW - q_index) <= WINDOW
    allowed = (in_window[None] & (query_docs[:, :, None] == key_docs[:, None, :]))[:, None, None]
    scores = jnp.einsum(
        "nqkgd,nskd->nkgqs", rotated_q, key_win, preferred_element_type=jnp.float32
    ) * HD ** (-0.5)
    masked = jnp.where(allowed, scores, -1e30)
    sink_col = sink_logit.reshape(kv_local, group_size)[None, :, :, None]
    top_score = jnp.maximum(jnp.max(masked, axis=-1), sink_col)
    exp_scores = jnp.where(allowed, jnp.exp(masked - top_score[..., None]), 0.0)
    denom_sum = jnp.sum(exp_scores, axis=-1) + jnp.exp(sink_col - top_score)
    probs = (exp_scores / denom_sum[..., None]).astype(jnp.bfloat16)
    attn = (
        jnp.einsum("nkgqs,nskd->nqkgd", probs, val_win, preferred_element_type=jnp.float32)
        .astype(jnp.bfloat16)
        .reshape(tok_count, q_local * HD)
    )
    partial_mix = jnp.dot(attn, out_proj, preferred_element_type=jnp.float32).astype(jnp.bfloat16)
    mixed = summed_on_arrival(partial_mix, "tp", 0)
    own_resid = lax.dynamic_slice_in_dim(residual, lax.axis_index("tp") * share_rows, share_rows, 0)
    after_mix = (own_resid.astype(jnp.float32) + rms_scale(mixed, gain_mix)).astype(jnp.bfloat16)
    own_normed = rms_scale(after_mix.astype(jnp.float32), gain_ffn_in).astype(jnp.bfloat16)
    normed = exchanged(jnp.broadcast_to(own_normed[None], (16, *own_normed.shape)))
    normed = normed.reshape(-1, 2048)
    across = (((1,), (1,)), ((), ()))
    ffn_part = 0.0
    for both in weights:
        up_acts = jnp.dot(normed, both[:, :256], preferred_element_type=jnp.float32)
        hidden = jnp.square(jax.nn.relu(up_acts)).astype(jnp.bfloat16)
        ffn_part += lax.dot_general(
            hidden, both[:, 256:], across, preferred_element_type=jnp.float32
        )
    arrived = exchanged(ffn_part.astype(jnp.bfloat16).reshape(16, -1, 2048))
    ffn_out = arrived.astype(jnp.float32).sum(axis=0)
    return (after_mix.astype(jnp.float32) + rms_scale(ffn_out, gain_ffn_out)).astype(jnp.bfloat16)


def solution(mesh):
    return jax.shard_map(
        body,
        mesh=mesh,
        in_specs=(
            P("sp", "tp"),
            P("sp", "tp"),
            P("sp", "tp"),
            P("tp"),
            P(),
            P("sp", None),
            P("tp", None),
            P(),
            P("sp", "tp"),
            P("tp", "sp"),
            P(),
            P(),
        ),
        out_specs=P(("sp", "tp"), None),
        check_vma=False,
    )
```

```python
import itertools

import jax
import jax.numpy as jnp
from jax import lax
from jax.sharding import PartitionSpec as P

HD = 128
WINDOW = 128


def device(z, y, x, core):
    return (4 * z + y) * 8 + 2 * x + core


def dealt(shard, turn):
    pairs = []
    for z, y, x, core in itertools.product(range(16), range(4), range(4), range(2)):
        target = core + 2 * ((y // 2 + turn) % 2)
        pairs.append((device(z, y, x, core), device(z, target, x, y % 2)))
    return lax.ppermute(shard, ("sp", "tp"), pairs)


def swapped(shard):
    return lax.ppermute(shard, "tp", [(i, i ^ 1) for i in range(8)])


def token_groups():
    return [
        [device(z, 2 * q + par, x, core) for par in range(2) for x in range(4)]
        for z in range(16)
        for q in range(2)
        for core in range(2)
    ]


def exchanged(pieces):
    return lax.all_to_all(
        pieces, ("sp", "tp"), 0, 0, axis_index_groups=token_groups(), tiled=True
    )


def halves(field, core):
    first, second = (field[:, 0], field[:, 1])
    return jnp.where(core == 0, first, second), jnp.where(core == 0, second, first)


def group_weights(up_proj, down_proj):
    both = jnp.concatenate([up_proj, down_proj.T], axis=1)
    same, other = (dealt(both, 0), dealt(both, 1))
    low = (lax.axis_index("sp") // 2) % 2 == 0
    rows = jnp.concatenate([jnp.where(low, same, other), jnp.where(low, other, same)], axis=0)
    along_z = [[4 * z + y for z in range(16)] for y in range(4)]
    own = lax.all_gather(rows, "sp", axis=0, tiled=True, axis_index_groups=along_z)
    return own, swapped(own)


def padded(shard, sides, width):
    for axis, dim in sides:
        devices, length = (lax.axis_size(axis), shard.shape[dim])
        up = [(i, (i + 1) % devices) for i in range(devices - 1)]
        down = [(j, i) for i, j in up]
        last = lax.slice_in_dim(shard, length - width, length, axis=dim)
        first = lax.slice_in_dim(shard, 0, width, axis=dim)
        before = lax.ppermute(last, axis, up)
        after = lax.ppermute(first, axis, down)
        shard = jnp.concatenate([before, shard, after], axis=dim)
    return shard


def split_up(shard, dim, devices):
    before, after = (shard.shape[:dim], shard.shape[dim + 1 :])
    return jnp.moveaxis(shard.reshape(*before, devices, -1, *after), dim, 0)


def summed_on_arrival(shard, axis, dim):
    pieces = split_up(shard, dim, lax.axis_size(axis))
    arrived = lax.all_to_all(pieces, axis, split_axis=0, concat_axis=0, tiled=True)
    return arrived.astype(jnp.float32).sum(axis=0)


def rotate(field, places):
    half_dim = HD // 2
    inv_freq = 10000.0 ** (-jnp.arange(0, HD, 2, dtype=jnp.float32) / HD)
    angles = places[:, None, None] * inv_freq[None, None, :]
    cosine = jnp.cos(angles)
    sine = jnp.sin(angles)
    lower = field[..., :half_dim].astype(jnp.float32)
    upper = field[..., half_dim:].astype(jnp.float32)
    return jnp.concatenate(
        [lower * cosine - upper * sine, upper * cosine + lower * sine], axis=-1
    ).astype(jnp.bfloat16)


def banded(field, blocks):
    framed = field.reshape((blocks + 2, WINDOW) + field.shape[1:])
    return jnp.concatenate([framed[:-2], framed[1:-1], framed[2:]], axis=1)


def rms_scale(field, gain_vec):
    return field * lax.rsqrt(jnp.mean(field * field, axis=-1, keepdims=True) + 1e-06) * gain_vec


def body(
    queries,
    key_heads,
    value_heads,
    sink_logit,
    doc_ids,
    residual,
    out_proj,
    gain_mix,
    up_proj,
    down_proj,
    gain_ffn_in,
    gain_ffn_out,
):
    tok_count = queries.shape[0]
    blocks = tok_count // WINDOW
    share_rows = tok_count // lax.axis_size("tp")
    q_local = queries.shape[1] // HD
    kv_local = key_heads.shape[1] // HD
    group_size = q_local // kv_local
    offset = lax.axis_index("sp") * tok_count
    own, other = group_weights(up_proj, down_proj)
    core = lax.axis_index("tp") % 2
    places = (offset + jnp.arange(tok_count)).astype(jnp.float32)
    rotated_q = rotate(queries.reshape(tok_count, q_local, HD), places).reshape(
        blocks, WINDOW, kv_local, group_size, HD
    )
    rotated_k = rotate(key_heads.reshape(tok_count, kv_local, HD), places).reshape(
        tok_count, kv_local * HD
    )
    rimmed = padded(jnp.stack([rotated_k, value_heads]), (("sp", 1),), WINDOW)
    key_win = banded(rimmed[0].reshape(-1, kv_local, HD), blocks)
    val_win = banded(rimmed[1].reshape(-1, kv_local, HD), blocks)
    padded_docs = jnp.pad(doc_ids, (WINDOW, WINDOW), constant_values=-1)
    key_docs = banded(lax.dynamic_slice_in_dim(padded_docs, offset, tok_count + 2 * WINDOW), blocks)
    query_docs = lax.dynamic_slice_in_dim(doc_ids, offset, tok_count).reshape(blocks, WINDOW)
    q_index = jnp.arange(WINDOW)[:, None]
    k_index = jnp.arange(3 * WINDOW)[None, :]
    in_window = jnp.abs(k_index - WINDOW - q_index) <= WINDOW
    allowed = (in_window[None] & (query_docs[:, :, None] == key_docs[:, None, :]))[:, None, None]
    scores = jnp.einsum(
        "nqkgd,nskd->nkgqs", rotated_q, key_win, preferred_element_type=jnp.float32
    ) * HD ** (-0.5)
    masked = jnp.where(allowed, scores, -1e30)
    sink_col = sink_logit.reshape(kv_local, group_size)[None, :, :, None]
    top_score = jnp.maximum(jnp.max(masked, axis=-1), sink_col)
    exp_scores = jnp.where(allowed, jnp.exp(masked - top_score[..., None]), 0.0)
    denom_sum = jnp.sum(exp_scores, axis=-1) + jnp.exp(sink_col - top_score)
    probs = (exp_scores / denom_sum[..., None]).astype(jnp.bfloat16)
    attn = (
        jnp.einsum("nkgqs,nskd->nqkgd", probs, val_win, preferred_element_type=jnp.float32)
        .astype(jnp.bfloat16)
        .reshape(tok_count, q_local * HD)
    )
    partial_mix = jnp.dot(attn, out_proj, preferred_element_type=jnp.float32).astype(jnp.bfloat16)
    mixed = summed_on_arrival(partial_mix, "tp", 0)
    own_resid = lax.dynamic_slice_in_dim(residual, lax.axis_index("tp") * share_rows, share_rows, 0)
    after_mix = (own_resid.astype(jnp.float32) + rms_scale(mixed, gain_mix)).astype(jnp.bfloat16)
    own_normed = rms_scale(after_mix.astype(jnp.float32), gain_ffn_in).astype(jnp.bfloat16)
    first, second = halves(own_normed.reshape(-1, 32, 2, 32).swapaxes(1, 2), core)
    ordered = jnp.concatenate([first.reshape(-1, 1024), second.reshape(-1, 1024)], axis=1)
    normed = exchanged(jnp.broadcast_to(ordered[None], (8, *ordered.shape)))
    normed = normed.reshape(-1, 2048)
    up_acts = jnp.dot(normed[:, :1024], own[:, :1024], preferred_element_type=jnp.float32)
    up_acts += jnp.dot(normed[:, 1024:], other[:, :1024], preferred_element_type=jnp.float32)
    hidden = jnp.square(jax.nn.relu(up_acts)).astype(jnp.bfloat16)
    across = (((1,), (1,)), ((), ()))
    parts = [
        lax.dot_general(hidden, w[:, 1024:], across, preferred_element_type=jnp.float32).astype(
            jnp.bfloat16
        )
        for w in (own, other)
    ]
    arrived = exchanged(jnp.concatenate(parts, axis=1).reshape(8, -1, 2048))
    summed = arrived.astype(jnp.float32).sum(axis=0).reshape(-1, 2, 32, 32)
    ffn_out = jnp.stack(halves(summed, core), axis=2).reshape(-1, 2048)
    return (after_mix.astype(jnp.float32) + rms_scale(ffn_out, gain_ffn_out)).astype(jnp.bfloat16)


def solution(mesh):
    return jax.shard_map(
        body,
        mesh=mesh,
        in_specs=(
            P("sp", "tp"),
            P("sp", "tp"),
            P("sp", "tp"),
            P("tp"),
            P(),
            P("sp", None),
            P("tp", None),
            P(),
            P("sp", "tp"),
            P("tp", "sp"),
            P(),
            P(),
        ),
        out_specs=P(("sp", "tp"), None),
        check_vma=False,
    )
```

```python
import jax
import jax.numpy as jnp
from jax import lax
from jax.sharding import PartitionSpec as P

HD = 128
WINDOW = 128


def device(z, y, x, core):
    return (4 * z + y) * 8 + 2 * x + core


def swapped(shard):
    return lax.ppermute(shard, "tp", [(i, i ^ 1) for i in range(8)])


def token_groups():
    return [
        [device(z, 2 * q + par, x, core) for par in range(2) for x in range(4)]
        for z in range(16)
        for q in range(2)
        for core in range(2)
    ]


def exchanged(pieces):
    return lax.all_to_all(
        pieces, ("sp", "tp"), 0, 0, axis_index_groups=token_groups(), tiled=True
    )


def group_weights(up_proj, down_proj):
    down_rows = down_proj.T
    halved = [
        jnp.concatenate([w[:, at : at + 512] for w in (up_proj, down_rows)], axis=1)
        for at in (0, 512)
    ]
    pieces = jnp.concatenate([jnp.broadcast_to(h[None], (4, 32, 1024)) for h in halved])
    rings = [
        [device(z, y, x, core) for core in range(2) for y in range(4)]
        for z in range(16)
        for x in range(4)
    ]
    dealt = lax.all_to_all(
        pieces, ("sp", "tp"), 0, 0, axis_index_groups=rings, tiled=True
    )
    block = lax.axis_index("sp") % 2
    rows = lax.dynamic_slice_in_dim(dealt, 4 * block, 4, axis=0).reshape(128, 1024)
    along_z = [[4 * z + y for z in range(16)] for y in range(4)]
    return lax.all_gather(rows, "sp", axis=0, tiled=True, axis_index_groups=along_z)


def ffn_up(normed, both):
    up_acts = jnp.dot(normed, both[:, :512], preferred_element_type=jnp.float32)
    return jnp.square(jax.nn.relu(up_acts)).astype(jnp.bfloat16)


def ffn_down(hidden, both):
    across = (((1,), (1,)), ((), ()))
    return lax.dot_general(hidden, both[:, 512:], across, preferred_element_type=jnp.float32)


def padded(shard, sides, width):
    for axis, dim in sides:
        devices, length = (lax.axis_size(axis), shard.shape[dim])
        up = [(i, (i + 1) % devices) for i in range(devices - 1)]
        down = [(j, i) for i, j in up]
        last = lax.slice_in_dim(shard, length - width, length, axis=dim)
        first = lax.slice_in_dim(shard, 0, width, axis=dim)
        before = lax.ppermute(last, axis, up)
        after = lax.ppermute(first, axis, down)
        shard = jnp.concatenate([before, shard, after], axis=dim)
    return shard


def split_up(shard, dim, devices):
    before, after = (shard.shape[:dim], shard.shape[dim + 1 :])
    return jnp.moveaxis(shard.reshape(*before, devices, -1, *after), dim, 0)


def summed_on_arrival(shard, axis, dim):
    pieces = split_up(shard, dim, lax.axis_size(axis))
    arrived = lax.all_to_all(pieces, axis, split_axis=0, concat_axis=0, tiled=True)
    return arrived.astype(jnp.float32).sum(axis=0)


def rotate(field, places):
    half_dim = HD // 2
    inv_freq = 10000.0 ** (-jnp.arange(0, HD, 2, dtype=jnp.float32) / HD)
    angles = places[:, None, None] * inv_freq[None, None, :]
    cosine = jnp.cos(angles)
    sine = jnp.sin(angles)
    lower = field[..., :half_dim].astype(jnp.float32)
    upper = field[..., half_dim:].astype(jnp.float32)
    return jnp.concatenate(
        [lower * cosine - upper * sine, upper * cosine + lower * sine], axis=-1
    ).astype(jnp.bfloat16)


def banded(field, blocks):
    framed = field.reshape((blocks + 2, WINDOW) + field.shape[1:])
    return jnp.concatenate([framed[:-2], framed[1:-1], framed[2:]], axis=1)


def rms_scale(field, gain_vec):
    return field * lax.rsqrt(jnp.mean(field * field, axis=-1, keepdims=True) + 1e-06) * gain_vec


def body(
    queries,
    key_heads,
    value_heads,
    sink_logit,
    doc_ids,
    residual,
    out_proj,
    gain_mix,
    up_proj,
    down_proj,
    gain_ffn_in,
    gain_ffn_out,
):
    tok_count = queries.shape[0]
    blocks = tok_count // WINDOW
    share_rows = tok_count // lax.axis_size("tp")
    q_local = queries.shape[1] // HD
    kv_local = key_heads.shape[1] // HD
    group_size = q_local // kv_local
    offset = lax.axis_index("sp") * tok_count
    weights = group_weights(up_proj, down_proj)
    places = (offset + jnp.arange(tok_count)).astype(jnp.float32)
    rotated_q = rotate(queries.reshape(tok_count, q_local, HD), places).reshape(
        blocks, WINDOW, kv_local, group_size, HD
    )
    rotated_k = rotate(key_heads.reshape(tok_count, kv_local, HD), places).reshape(
        tok_count, kv_local * HD
    )
    rimmed = padded(jnp.stack([rotated_k, value_heads]), (("sp", 1),), WINDOW)
    key_win = banded(rimmed[0].reshape(-1, kv_local, HD), blocks)
    val_win = banded(rimmed[1].reshape(-1, kv_local, HD), blocks)
    padded_docs = jnp.pad(doc_ids, (WINDOW, WINDOW), constant_values=-1)
    key_docs = banded(lax.dynamic_slice_in_dim(padded_docs, offset, tok_count + 2 * WINDOW), blocks)
    query_docs = lax.dynamic_slice_in_dim(doc_ids, offset, tok_count).reshape(blocks, WINDOW)
    q_index = jnp.arange(WINDOW)[:, None]
    k_index = jnp.arange(3 * WINDOW)[None, :]
    in_window = jnp.abs(k_index - WINDOW - q_index) <= WINDOW
    allowed = (in_window[None] & (query_docs[:, :, None] == key_docs[:, None, :]))[:, None, None]
    scores = jnp.einsum(
        "nqkgd,nskd->nkgqs", rotated_q, key_win, preferred_element_type=jnp.float32
    ) * HD ** (-0.5)
    masked = jnp.where(allowed, scores, -1e30)
    sink_col = sink_logit.reshape(kv_local, group_size)[None, :, :, None]
    top_score = jnp.maximum(jnp.max(masked, axis=-1), sink_col)
    exp_scores = jnp.where(allowed, jnp.exp(masked - top_score[..., None]), 0.0)
    denom_sum = jnp.sum(exp_scores, axis=-1) + jnp.exp(sink_col - top_score)
    probs = (exp_scores / denom_sum[..., None]).astype(jnp.bfloat16)
    attn = (
        jnp.einsum("nkgqs,nskd->nqkgd", probs, val_win, preferred_element_type=jnp.float32)
        .astype(jnp.bfloat16)
        .reshape(tok_count, q_local * HD)
    )
    partial_mix = jnp.dot(attn, out_proj, preferred_element_type=jnp.float32).astype(jnp.bfloat16)
    mixed = summed_on_arrival(partial_mix, "tp", 0)
    own_resid = lax.dynamic_slice_in_dim(residual, lax.axis_index("tp") * share_rows, share_rows, 0)
    after_mix = (own_resid.astype(jnp.float32) + rms_scale(mixed, gain_mix)).astype(jnp.bfloat16)
    own_normed = rms_scale(after_mix.astype(jnp.float32), gain_ffn_in).astype(jnp.bfloat16)
    normed = exchanged(jnp.broadcast_to(own_normed[None], (8, *own_normed.shape)))
    normed = normed.reshape(-1, 2048)
    other_normed = swapped(normed)
    other_part = ffn_down(ffn_up(other_normed, weights), weights).astype(jnp.bfloat16)
    received = swapped(other_part)
    hidden = lax.optimization_barrier(ffn_up(normed, weights))
    own_part = ffn_down(hidden, weights)
    both_parts = (own_part + received.astype(jnp.float32)).astype(jnp.bfloat16)
    ffn_out = exchanged(both_parts.reshape(8, -1, 2048)).astype(jnp.float32).sum(axis=0)
    return (after_mix.astype(jnp.float32) + rms_scale(ffn_out, gain_ffn_out)).astype(jnp.bfloat16)


def solution(mesh):
    return jax.shard_map(
        body,
        mesh=mesh,
        in_specs=(
            P("sp", "tp"),
            P("sp", "tp"),
            P("sp", "tp"),
            P("tp"),
            P(),
            P("sp", None),
            P("tp", None),
            P(),
            P("sp", "tp"),
            P("tp", "sp"),
            P(),
            P(),
        ),
        out_specs=P(("sp", "tp"), None),
        check_vma=False,
    )
```

```python
import itertools

import jax
import jax.numpy as jnp
from jax import lax
from jax.sharding import PartitionSpec as P

HD = 128
WINDOW = 128


def device(z, y, x, core):
    return (4 * z + y) * 8 + 2 * x + core


def swapped(shard):
    return lax.ppermute(shard, "tp", [(i, i ^ 1) for i in range(8)])


def token_groups():
    return [
        [device(z, 2 * q + par, x, core) for par in range(2) for x in range(4)]
        for z in range(16)
        for q in range(2)
        for core in range(2)
    ]


def exchanged(pieces):
    return lax.all_to_all(
        pieces, ("sp", "tp"), 0, 0, axis_index_groups=token_groups(), tiled=True
    )


def dealt(shard, turn_y, turn_core):
    pairs = []
    for z, y, x, core in itertools.product(range(16), range(4), range(4), range(2)):
        target = device(z, core + 2 * ((y // 2 + turn_y) % 2), x, (y + turn_core) % 2)
        pairs.append((device(z, y, x, core), target))
    return lax.ppermute(shard, ("sp", "tp"), pairs)


def in_order(swap, first, second):
    return [jnp.where(swap, second, first), jnp.where(swap, first, second)]


def group_weights(up_proj, down_proj):
    y, core = (lax.axis_index("sp") % 4, lax.axis_index("tp") % 2)
    down_rows = down_proj.T
    halved = [
        jnp.concatenate([w[:, at : at + 512] for w in (up_proj, down_rows)], axis=1)
        for at in (0, 512)
    ]
    sent = in_order(y % 2 == 1, *halved)
    got = [[dealt(sent[b], a, b) for b in range(2)] for a in range(2)]
    got = [in_order(core == 1, *pair) for pair in got]
    low, high = ([in_order(y >= 2, got[0][b], got[1][b])[a] for b in range(2)] for a in range(2))
    rows = jnp.concatenate(low + high, axis=0)
    along_z = [[4 * z + y for z in range(16)] for y in range(4)]
    return lax.all_gather(rows, "sp", axis=0, tiled=True, axis_index_groups=along_z)


def ffn_up(normed, both):
    up_acts = jnp.dot(normed, both[:, :512], preferred_element_type=jnp.float32)
    return jnp.square(jax.nn.relu(up_acts)).astype(jnp.bfloat16)


def ffn_down(hidden, both):
    across = (((1,), (1,)), ((), ()))
    return lax.dot_general(hidden, both[:, 512:], across, preferred_element_type=jnp.float32)


def padded(shard, sides, width):
    for axis, dim in sides:
        devices, length = (lax.axis_size(axis), shard.shape[dim])
        up = [(i, (i + 1) % devices) for i in range(devices - 1)]
        down = [(j, i) for i, j in up]
        last = lax.slice_in_dim(shard, length - width, length, axis=dim)
        first = lax.slice_in_dim(shard, 0, width, axis=dim)
        before = lax.ppermute(last, axis, up)
        after = lax.ppermute(first, axis, down)
        shard = jnp.concatenate([before, shard, after], axis=dim)
    return shard


def split_up(shard, dim, devices):
    before, after = (shard.shape[:dim], shard.shape[dim + 1 :])
    return jnp.moveaxis(shard.reshape(*before, devices, -1, *after), dim, 0)


def summed_on_arrival(shard, axis, dim):
    pieces = split_up(shard, dim, lax.axis_size(axis))
    arrived = lax.all_to_all(pieces, axis, split_axis=0, concat_axis=0, tiled=True)
    return arrived.astype(jnp.float32).sum(axis=0)


def rotate(field, places):
    half_dim = HD // 2
    inv_freq = 10000.0 ** (-jnp.arange(0, HD, 2, dtype=jnp.float32) / HD)
    angles = places[:, None, None] * inv_freq[None, None, :]
    cosine = jnp.cos(angles)
    sine = jnp.sin(angles)
    lower = field[..., :half_dim].astype(jnp.float32)
    upper = field[..., half_dim:].astype(jnp.float32)
    return jnp.concatenate(
        [lower * cosine - upper * sine, upper * cosine + lower * sine], axis=-1
    ).astype(jnp.bfloat16)


def banded(field, blocks):
    framed = field.reshape((blocks + 2, WINDOW) + field.shape[1:])
    return jnp.concatenate([framed[:-2], framed[1:-1], framed[2:]], axis=1)


def rms_scale(field, gain_vec):
    return field * lax.rsqrt(jnp.mean(field * field, axis=-1, keepdims=True) + 1e-06) * gain_vec


def body(
    queries,
    key_heads,
    value_heads,
    sink_logit,
    doc_ids,
    residual,
    out_proj,
    gain_mix,
    up_proj,
    down_proj,
    gain_ffn_in,
    gain_ffn_out,
):
    tok_count = queries.shape[0]
    blocks = tok_count // WINDOW
    share_rows = tok_count // lax.axis_size("tp")
    q_local = queries.shape[1] // HD
    kv_local = key_heads.shape[1] // HD
    group_size = q_local // kv_local
    offset = lax.axis_index("sp") * tok_count
    weights = group_weights(up_proj, down_proj)
    places = (offset + jnp.arange(tok_count)).astype(jnp.float32)
    rotated_q = rotate(queries.reshape(tok_count, q_local, HD), places).reshape(
        blocks, WINDOW, kv_local, group_size, HD
    )
    rotated_k = rotate(key_heads.reshape(tok_count, kv_local, HD), places).reshape(
        tok_count, kv_local * HD
    )
    rimmed = padded(jnp.stack([rotated_k, value_heads]), (("sp", 1),), WINDOW)
    key_win = banded(rimmed[0].reshape(-1, kv_local, HD), blocks)
    val_win = banded(rimmed[1].reshape(-1, kv_local, HD), blocks)
    padded_docs = jnp.pad(doc_ids, (WINDOW, WINDOW), constant_values=-1)
    key_docs = banded(lax.dynamic_slice_in_dim(padded_docs, offset, tok_count + 2 * WINDOW), blocks)
    query_docs = lax.dynamic_slice_in_dim(doc_ids, offset, tok_count).reshape(blocks, WINDOW)
    q_index = jnp.arange(WINDOW)[:, None]
    k_index = jnp.arange(3 * WINDOW)[None, :]
    in_window = jnp.abs(k_index - WINDOW - q_index) <= WINDOW
    allowed = (in_window[None] & (query_docs[:, :, None] == key_docs[:, None, :]))[:, None, None]
    scores = jnp.einsum(
        "nqkgd,nskd->nkgqs", rotated_q, key_win, preferred_element_type=jnp.float32
    ) * HD ** (-0.5)
    masked = jnp.where(allowed, scores, -1e30)
    sink_col = sink_logit.reshape(kv_local, group_size)[None, :, :, None]
    top_score = jnp.maximum(jnp.max(masked, axis=-1), sink_col)
    exp_scores = jnp.where(allowed, jnp.exp(masked - top_score[..., None]), 0.0)
    denom_sum = jnp.sum(exp_scores, axis=-1) + jnp.exp(sink_col - top_score)
    probs = (exp_scores / denom_sum[..., None]).astype(jnp.bfloat16)
    attn = (
        jnp.einsum("nkgqs,nskd->nqkgd", probs, val_win, preferred_element_type=jnp.float32)
        .astype(jnp.bfloat16)
        .reshape(tok_count, q_local * HD)
    )
    partial_mix = jnp.dot(attn, out_proj, preferred_element_type=jnp.float32).astype(jnp.bfloat16)
    mixed = summed_on_arrival(partial_mix, "tp", 0)
    own_resid = lax.dynamic_slice_in_dim(residual, lax.axis_index("tp") * share_rows, share_rows, 0)
    after_mix = (own_resid.astype(jnp.float32) + rms_scale(mixed, gain_mix)).astype(jnp.bfloat16)
    own_normed = rms_scale(after_mix.astype(jnp.float32), gain_ffn_in).astype(jnp.bfloat16)
    normed = exchanged(jnp.broadcast_to(own_normed[None], (8, *own_normed.shape)))
    normed = normed.reshape(-1, 2048)
    other_normed = swapped(normed)
    other_part = ffn_down(ffn_up(other_normed, weights), weights).astype(jnp.bfloat16)
    received = swapped(other_part)
    hidden = lax.optimization_barrier(ffn_up(normed, weights))
    own_part = ffn_down(hidden, weights)
    both_parts = (own_part + received.astype(jnp.float32)).astype(jnp.bfloat16)
    ffn_out = exchanged(both_parts.reshape(8, -1, 2048)).astype(jnp.float32).sum(axis=0)
    return (after_mix.astype(jnp.float32) + rms_scale(ffn_out, gain_ffn_out)).astype(jnp.bfloat16)


def solution(mesh):
    return jax.shard_map(
        body,
        mesh=mesh,
        in_specs=(
            P("sp", "tp"),
            P("sp", "tp"),
            P("sp", "tp"),
            P("tp"),
            P(),
            P("sp", None),
            P("tp", None),
            P(),
            P("sp", "tp"),
            P("tp", "sp"),
            P(),
            P(),
        ),
        out_specs=P(("sp", "tp"), None),
        check_vma=False,
    )
```

```python
import jax
import jax.numpy as jnp
from jax import lax
from jax.sharding import PartitionSpec as P

HD = 128
WINDOW = 128


def device(z, y, x, core):
    return (4 * z + y) * 8 + 2 * x + core


def swapped(shard):
    return lax.ppermute(shard, "tp", [(i, i ^ 1) for i in range(8)])


def token_groups():
    return [
        [device(z, 2 * q + par, x, core) for par in range(2) for x in range(4)]
        for z in range(16)
        for q in range(2)
        for core in range(2)
    ]


def exchanged(pieces):
    return lax.all_to_all(
        pieces, ("sp", "tp"), 0, 0, axis_index_groups=token_groups(), tiled=True
    )


def group_weights(up_proj, down_proj):
    down_rows = down_proj.T
    halved = [
        jnp.concatenate([w[:, at : at + 512] for w in (up_proj, down_rows)], axis=1)
        for at in (0, 512)
    ]
    along_y = [[4 * z + y for y in range(4)] for z in range(16)]
    along_z = [[4 * z + y for z in range(16)] for y in range(4)]
    rows = lax.all_to_all(jnp.stack(halved * 2), "sp", 0, 0, axis_index_groups=along_y, tiled=True)
    return lax.all_gather(
        rows.reshape(128, 1024), "sp", axis=0, tiled=True, axis_index_groups=along_z
    )


def ffn_up(normed, both):
    up_acts = jnp.dot(normed, both[:, :512], preferred_element_type=jnp.float32)
    return jnp.square(jax.nn.relu(up_acts)).astype(jnp.bfloat16)


def ffn_down(hidden, both):
    across = (((1,), (1,)), ((), ()))
    return lax.dot_general(hidden, both[:, 512:], across, preferred_element_type=jnp.float32)


def padded(shard, sides, width):
    for axis, dim in sides:
        devices, length = (lax.axis_size(axis), shard.shape[dim])
        up = [(i, (i + 1) % devices) for i in range(devices - 1)]
        down = [(j, i) for i, j in up]
        last = lax.slice_in_dim(shard, length - width, length, axis=dim)
        first = lax.slice_in_dim(shard, 0, width, axis=dim)
        before = lax.ppermute(last, axis, up)
        after = lax.ppermute(first, axis, down)
        shard = jnp.concatenate([before, shard, after], axis=dim)
    return shard


def split_up(shard, dim, devices):
    before, after = (shard.shape[:dim], shard.shape[dim + 1 :])
    return jnp.moveaxis(shard.reshape(*before, devices, -1, *after), dim, 0)


def summed_on_arrival(shard, axis, dim):
    pieces = split_up(shard, dim, lax.axis_size(axis))
    arrived = lax.all_to_all(pieces, axis, split_axis=0, concat_axis=0, tiled=True)
    return arrived.astype(jnp.float32).sum(axis=0)


def rotate(field, places):
    half_dim = HD // 2
    inv_freq = 10000.0 ** (-jnp.arange(0, HD, 2, dtype=jnp.float32) / HD)
    angles = places[:, None, None] * inv_freq[None, None, :]
    cosine = jnp.cos(angles)
    sine = jnp.sin(angles)
    lower = field[..., :half_dim].astype(jnp.float32)
    upper = field[..., half_dim:].astype(jnp.float32)
    return jnp.concatenate(
        [lower * cosine - upper * sine, upper * cosine + lower * sine], axis=-1
    ).astype(jnp.bfloat16)


def banded(field, blocks):
    framed = field.reshape((blocks + 2, WINDOW) + field.shape[1:])
    return jnp.concatenate([framed[:-2], framed[1:-1], framed[2:]], axis=1)


def rms_scale(field, gain_vec):
    return field * lax.rsqrt(jnp.mean(field * field, axis=-1, keepdims=True) + 1e-06) * gain_vec


def body(
    queries,
    key_heads,
    value_heads,
    sink_logit,
    doc_ids,
    residual,
    out_proj,
    gain_mix,
    up_proj,
    down_proj,
    gain_ffn_in,
    gain_ffn_out,
):
    tok_count = queries.shape[0]
    blocks = tok_count // WINDOW
    share_rows = tok_count // lax.axis_size("tp")
    q_local = queries.shape[1] // HD
    kv_local = key_heads.shape[1] // HD
    group_size = q_local // kv_local
    offset = lax.axis_index("sp") * tok_count
    weights = group_weights(up_proj, down_proj)
    places = (offset + jnp.arange(tok_count)).astype(jnp.float32)
    rotated_q = rotate(queries.reshape(tok_count, q_local, HD), places).reshape(
        blocks, WINDOW, kv_local, group_size, HD
    )
    rotated_k = rotate(key_heads.reshape(tok_count, kv_local, HD), places).reshape(
        tok_count, kv_local * HD
    )
    rimmed = padded(jnp.stack([rotated_k, value_heads]), (("sp", 1),), WINDOW)
    key_win = banded(rimmed[0].reshape(-1, kv_local, HD), blocks)
    val_win = banded(rimmed[1].reshape(-1, kv_local, HD), blocks)
    padded_docs = jnp.pad(doc_ids, (WINDOW, WINDOW), constant_values=-1)
    key_docs = banded(lax.dynamic_slice_in_dim(padded_docs, offset, tok_count + 2 * WINDOW), blocks)
    query_docs = lax.dynamic_slice_in_dim(doc_ids, offset, tok_count).reshape(blocks, WINDOW)
    q_index = jnp.arange(WINDOW)[:, None]
    k_index = jnp.arange(3 * WINDOW)[None, :]
    in_window = jnp.abs(k_index - WINDOW - q_index) <= WINDOW
    allowed = (in_window[None] & (query_docs[:, :, None] == key_docs[:, None, :]))[:, None, None]
    scores = jnp.einsum(
        "nqkgd,nskd->nkgqs", rotated_q, key_win, preferred_element_type=jnp.float32
    ) * HD ** (-0.5)
    masked = jnp.where(allowed, scores, -1e30)
    sink_col = sink_logit.reshape(kv_local, group_size)[None, :, :, None]
    top_score = jnp.maximum(jnp.max(masked, axis=-1), sink_col)
    exp_scores = jnp.where(allowed, jnp.exp(masked - top_score[..., None]), 0.0)
    denom_sum = jnp.sum(exp_scores, axis=-1) + jnp.exp(sink_col - top_score)
    probs = (exp_scores / denom_sum[..., None]).astype(jnp.bfloat16)
    attn = (
        jnp.einsum("nkgqs,nskd->nqkgd", probs, val_win, preferred_element_type=jnp.float32)
        .astype(jnp.bfloat16)
        .reshape(tok_count, q_local * HD)
    )
    partial_mix = jnp.dot(attn, out_proj, preferred_element_type=jnp.float32).astype(jnp.bfloat16)
    mixed = summed_on_arrival(partial_mix, "tp", 0)
    own_resid = lax.dynamic_slice_in_dim(residual, lax.axis_index("tp") * share_rows, share_rows, 0)
    after_mix = (own_resid.astype(jnp.float32) + rms_scale(mixed, gain_mix)).astype(jnp.bfloat16)
    own_normed = rms_scale(after_mix.astype(jnp.float32), gain_ffn_in).astype(jnp.bfloat16)
    normed = exchanged(jnp.broadcast_to(own_normed[None], (8, *own_normed.shape)))
    normed = normed.reshape(-1, 2048)
    other_normed = swapped(normed)
    other_part = ffn_down(ffn_up(other_normed, weights), weights).astype(jnp.bfloat16)
    received = swapped(other_part)
    hidden = lax.optimization_barrier(ffn_up(normed, weights))
    own_part = ffn_down(hidden, weights)
    both_parts = (own_part + received.astype(jnp.float32)).astype(jnp.bfloat16)
    ffn_out = exchanged(both_parts.reshape(8, -1, 2048)).astype(jnp.float32).sum(axis=0)
    return (after_mix.astype(jnp.float32) + rms_scale(ffn_out, gain_ffn_out)).astype(jnp.bfloat16)


def solution(mesh):
    return jax.shard_map(
        body,
        mesh=mesh,
        in_specs=(
            P("sp", "tp"),
            P("sp", "tp"),
            P("sp", "tp"),
            P("tp"),
            P(),
            P("sp", None),
            P("tp", None),
            P(),
            P("sp", "tp"),
            P("tp", "sp"),
            P(),
            P(),
        ),
        out_specs=P(("sp", "tp"), None),
        check_vma=False,
    )
```

```python
import jax
import jax.numpy as jnp
from jax import lax
from jax.experimental import pallas as pl
from jax.experimental.pallas import tpu as pltpu
from jax.sharding import PartitionSpec as P

HD = 128
WINDOW = 128
CHUNKS = 4


def device(z, y, x, core):
    return (4 * z + y) * 8 + 2 * x + core


def swapped(shard):
    return lax.ppermute(shard, "tp", [(i, i ^ 1) for i in range(8)])


def token_groups():
    return [
        [device(z, 2 * q + par, x, core) for par in range(2) for x in range(4)]
        for z in range(16)
        for q in range(2)
        for core in range(2)
    ]


def exchanged(pieces):
    return lax.all_to_all(
        pieces, ("sp", "tp"), 0, 0, axis_index_groups=token_groups(), tiled=True
    )


def group_weights(up_proj, down_proj):
    down_rows = down_proj.T
    halved = [
        jnp.concatenate([w[:, at : at + 512] for w in (up_proj, down_rows)], axis=1)
        for at in (0, 512)
    ]
    along_y = [[4 * z + y for y in range(4)] for z in range(16)]
    along_z = [[4 * z + y for z in range(16)] for y in range(4)]
    rows = lax.all_to_all(jnp.stack(halved * 2), "sp", 0, 0, axis_index_groups=along_y, tiled=True)
    return lax.all_gather(
        rows.reshape(128, 1024), "sp", axis=0, tiled=True, axis_index_groups=along_z
    )


def ffn_up(normed, both):
    up_acts = jnp.dot(normed, both[:, :512], preferred_element_type=jnp.float32)
    return jnp.square(jax.nn.relu(up_acts)).astype(jnp.bfloat16)


def ffn_down(hidden, both):
    across = (((1,), (1,)), ((), ()))
    return lax.dot_general(hidden, both[:, 512:], across, preferred_element_type=jnp.float32)


def ffn_kernel(tokens, both, out, held, arrivals):
    chunks = arrivals.shape[0]
    size = held.shape[0] // chunks
    half = held.shape[1] // 2
    spans = [pl.ds(k * size, size) for k in range(chunks)]
    copies = [
        pltpu.make_async_copy(both.at[span], held.at[span], arrivals.at[k])
        for k, span in enumerate(spans)
    ]
    for copy in copies:
        copy.start()
    up_acts = jnp.zeros((tokens.shape[0], half), jnp.float32)
    for copy, span in zip(copies, spans):
        copy.wait()
        up_acts += jnp.dot(
            tokens[:, span], held[span, :half], preferred_element_type=jnp.float32
        )
    hidden = jnp.square(jax.nn.relu(up_acts)).astype(jnp.bfloat16)
    for span in spans:
        out[:, span] = lax.dot_general(
            hidden,
            held[span, half:],
            (((1,), (1,)), ((), ())),
            preferred_element_type=jnp.float32,
        ).astype(jnp.bfloat16)


def ffn_in_kernel(tokens, both):
    return pl.pallas_call(
        ffn_kernel,
        out_shape=jax.ShapeDtypeStruct(tokens.shape, jnp.bfloat16),
        in_specs=[
            pl.BlockSpec(memory_space=pltpu.VMEM),
            pl.BlockSpec(memory_space=pl.ANY),
        ],
        out_specs=pl.BlockSpec(memory_space=pltpu.VMEM),
        scratch_shapes=[
            pltpu.VMEM(both.shape, jnp.bfloat16),
            pltpu.SemaphoreType.DMA((CHUNKS,)),
        ],
        cost_estimate=pl.CostEstimate(
            flops=2 * 384 * 2048 * 1024, bytes_accessed=7 << 20, transcendentals=0
        ),
        name="ffn_other",
    )(tokens, both)


def padded(shard, sides, width):
    for axis, dim in sides:
        devices, length = (lax.axis_size(axis), shard.shape[dim])
        up = [(i, (i + 1) % devices) for i in range(devices - 1)]
        down = [(j, i) for i, j in up]
        last = lax.slice_in_dim(shard, length - width, length, axis=dim)
        first = lax.slice_in_dim(shard, 0, width, axis=dim)
        before = lax.ppermute(last, axis, up)
        after = lax.ppermute(first, axis, down)
        shard = jnp.concatenate([before, shard, after], axis=dim)
    return shard


def split_up(shard, dim, devices):
    before, after = (shard.shape[:dim], shard.shape[dim + 1 :])
    return jnp.moveaxis(shard.reshape(*before, devices, -1, *after), dim, 0)


def summed_on_arrival(shard, axis, dim):
    pieces = split_up(shard, dim, lax.axis_size(axis))
    arrived = lax.all_to_all(pieces, axis, split_axis=0, concat_axis=0, tiled=True)
    return arrived.astype(jnp.float32).sum(axis=0)


def rotate(field, places):
    half_dim = HD // 2
    inv_freq = 10000.0 ** (-jnp.arange(0, HD, 2, dtype=jnp.float32) / HD)
    angles = places[:, None, None] * inv_freq[None, None, :]
    cosine = jnp.cos(angles)
    sine = jnp.sin(angles)
    lower = field[..., :half_dim].astype(jnp.float32)
    upper = field[..., half_dim:].astype(jnp.float32)
    return jnp.concatenate(
        [lower * cosine - upper * sine, upper * cosine + lower * sine], axis=-1
    ).astype(jnp.bfloat16)


def banded(field, blocks):
    framed = field.reshape((blocks + 2, WINDOW) + field.shape[1:])
    return jnp.concatenate([framed[:-2], framed[1:-1], framed[2:]], axis=1)


def rms_scale(field, gain_vec):
    return field * lax.rsqrt(jnp.mean(field * field, axis=-1, keepdims=True) + 1e-06) * gain_vec


def body(
    queries,
    key_heads,
    value_heads,
    sink_logit,
    doc_ids,
    residual,
    out_proj,
    gain_mix,
    up_proj,
    down_proj,
    gain_ffn_in,
    gain_ffn_out,
):
    tok_count = queries.shape[0]
    blocks = tok_count // WINDOW
    share_rows = tok_count // lax.axis_size("tp")
    q_local = queries.shape[1] // HD
    kv_local = key_heads.shape[1] // HD
    group_size = q_local // kv_local
    offset = lax.axis_index("sp") * tok_count
    weights = group_weights(up_proj, down_proj)
    places = (offset + jnp.arange(tok_count)).astype(jnp.float32)
    rotated_q = rotate(queries.reshape(tok_count, q_local, HD), places).reshape(
        blocks, WINDOW, kv_local, group_size, HD
    )
    rotated_k = rotate(key_heads.reshape(tok_count, kv_local, HD), places).reshape(
        tok_count, kv_local * HD
    )
    rimmed = padded(jnp.stack([rotated_k, value_heads]), (("sp", 1),), WINDOW)
    key_win = banded(rimmed[0].reshape(-1, kv_local, HD), blocks)
    val_win = banded(rimmed[1].reshape(-1, kv_local, HD), blocks)
    padded_docs = jnp.pad(doc_ids, (WINDOW, WINDOW), constant_values=-1)
    key_docs = banded(lax.dynamic_slice_in_dim(padded_docs, offset, tok_count + 2 * WINDOW), blocks)
    query_docs = lax.dynamic_slice_in_dim(doc_ids, offset, tok_count).reshape(blocks, WINDOW)
    q_index = jnp.arange(WINDOW)[:, None]
    k_index = jnp.arange(3 * WINDOW)[None, :]
    in_window = jnp.abs(k_index - WINDOW - q_index) <= WINDOW
    allowed = (in_window[None] & (query_docs[:, :, None] == key_docs[:, None, :]))[:, None, None]
    scores = jnp.einsum(
        "nqkgd,nskd->nkgqs", rotated_q, key_win, preferred_element_type=jnp.float32
    ) * HD ** (-0.5)
    masked = jnp.where(allowed, scores, -1e30)
    sink_col = sink_logit.reshape(kv_local, group_size)[None, :, :, None]
    top_score = jnp.maximum(jnp.max(masked, axis=-1), sink_col)
    exp_scores = jnp.where(allowed, jnp.exp(masked - top_score[..., None]), 0.0)
    denom_sum = jnp.sum(exp_scores, axis=-1) + jnp.exp(sink_col - top_score)
    probs = (exp_scores / denom_sum[..., None]).astype(jnp.bfloat16)
    attn = (
        jnp.einsum("nkgqs,nskd->nqkgd", probs, val_win, preferred_element_type=jnp.float32)
        .astype(jnp.bfloat16)
        .reshape(tok_count, q_local * HD)
    )
    partial_mix = jnp.dot(attn, out_proj, preferred_element_type=jnp.float32).astype(jnp.bfloat16)
    mixed = summed_on_arrival(partial_mix, "tp", 0)
    own_resid = lax.dynamic_slice_in_dim(residual, lax.axis_index("tp") * share_rows, share_rows, 0)
    after_mix = (own_resid.astype(jnp.float32) + rms_scale(mixed, gain_mix)).astype(jnp.bfloat16)
    own_normed = rms_scale(after_mix.astype(jnp.float32), gain_ffn_in).astype(jnp.bfloat16)
    normed = exchanged(jnp.broadcast_to(own_normed[None], (8, *own_normed.shape)))
    normed = normed.reshape(-1, 2048)
    other_normed = swapped(normed)
    other_part = ffn_in_kernel(other_normed, weights)
    received = swapped(other_part)
    hidden = lax.optimization_barrier(ffn_up(normed, weights))
    own_part = ffn_down(hidden, weights)
    both_parts = (own_part + received.astype(jnp.float32)).astype(jnp.bfloat16)
    ffn_out = exchanged(both_parts.reshape(8, -1, 2048)).astype(jnp.float32).sum(axis=0)
    return (after_mix.astype(jnp.float32) + rms_scale(ffn_out, gain_ffn_out)).astype(jnp.bfloat16)


def solution(mesh):
    return jax.shard_map(
        body,
        mesh=mesh,
        in_specs=(
            P("sp", "tp"),
            P("sp", "tp"),
            P("sp", "tp"),
            P("tp"),
            P(),
            P("sp", None),
            P("tp", None),
            P(),
            P("sp", "tp"),
            P("tp", "sp"),
            P(),
            P(),
        ),
        out_specs=P(("sp", "tp"), None),
        check_vma=False,
    )
```

```python
import jax
import jax.numpy as jnp
from jax import lax
from jax.sharding import PartitionSpec as P

HD = 128
WINDOW = 128


def device(z, y, x, core):
    return (4 * z + y) * 8 + 2 * x + core


def swapped(shard):
    return lax.ppermute(shard, "tp", [(i, i ^ 1) for i in range(8)])


def token_groups():
    return [
        [device(z, 2 * q + par, x, core) for par in range(2) for x in range(4)]
        for z in range(16)
        for q in range(2)
        for core in range(2)
    ]


def exchanged(pieces):
    return lax.all_to_all(
        pieces, ("sp", "tp"), 0, 0, axis_index_groups=token_groups(), tiled=True
    )


def group_weights(up_proj, down_proj):
    down_rows = down_proj.T
    halved = [
        jnp.concatenate([w[:, at : at + 512] for w in (up_proj, down_rows)], axis=1)
        for at in (0, 512)
    ]
    along_y = [[4 * z + y for y in range(4)] for z in range(16)]
    along_z = [[4 * z + y for z in range(16)] for y in range(4)]
    rows = lax.all_to_all(jnp.stack(halved * 2), "sp", 0, 0, axis_index_groups=along_y, tiled=True)
    return lax.all_gather(
        rows.reshape(128, 1024), "sp", axis=0, tiled=True, axis_index_groups=along_z
    )


def ffn_up(normed, both):
    up_acts = jnp.dot(normed, both[:, :512], preferred_element_type=jnp.float32)
    return jnp.square(jax.nn.relu(up_acts)).astype(jnp.bfloat16)


def ffn_down(hidden, both):
    across = (((1,), (1,)), ((), ()))
    return lax.dot_general(hidden, both[:, 512:], across, preferred_element_type=jnp.float32)


def padded(shard, sides, width):
    for axis, dim in sides:
        devices, length = (lax.axis_size(axis), shard.shape[dim])
        up = [(i, (i + 1) % devices) for i in range(devices - 1)]
        down = [(j, i) for i, j in up]
        last = lax.slice_in_dim(shard, length - width, length, axis=dim)
        first = lax.slice_in_dim(shard, 0, width, axis=dim)
        before = lax.ppermute(last, axis, up)
        after = lax.ppermute(first, axis, down)
        shard = jnp.concatenate([before, shard, after], axis=dim)
    return shard


def split_up(shard, dim, devices):
    before, after = (shard.shape[:dim], shard.shape[dim + 1 :])
    return jnp.moveaxis(shard.reshape(*before, devices, -1, *after), dim, 0)


def summed_on_arrival(shard, axis, dim):
    pieces = split_up(shard, dim, lax.axis_size(axis))
    arrived = lax.all_to_all(pieces, axis, split_axis=0, concat_axis=0, tiled=True)
    return arrived.astype(jnp.float32).sum(axis=0)


def rotate(field, places):
    half_dim = HD // 2
    inv_freq = 10000.0 ** (-jnp.arange(0, HD, 2, dtype=jnp.float32) / HD)
    angles = places[:, None, None] * inv_freq[None, None, :]
    cosine = jnp.cos(angles)
    sine = jnp.sin(angles)
    lower = field[..., :half_dim].astype(jnp.float32)
    upper = field[..., half_dim:].astype(jnp.float32)
    return jnp.concatenate(
        [lower * cosine - upper * sine, upper * cosine + lower * sine], axis=-1
    ).astype(jnp.bfloat16)


def banded(field, blocks):
    framed = field.reshape((blocks + 2, WINDOW) + field.shape[1:])
    return jnp.concatenate([framed[:-2], framed[1:-1], framed[2:]], axis=1)


def rms_scale(field, gain_vec):
    return field * lax.rsqrt(jnp.mean(field * field, axis=-1, keepdims=True) + 1e-06) * gain_vec


def body(
    queries,
    key_heads,
    value_heads,
    sink_logit,
    doc_ids,
    residual,
    out_proj,
    gain_mix,
    up_proj,
    down_proj,
    gain_ffn_in,
    gain_ffn_out,
):
    tok_count = queries.shape[0]
    blocks = tok_count // WINDOW
    share_rows = tok_count // lax.axis_size("tp")
    q_local = queries.shape[1] // HD
    kv_local = key_heads.shape[1] // HD
    group_size = q_local // kv_local
    offset = lax.axis_index("sp") * tok_count
    weights = group_weights(up_proj, down_proj)
    places = (offset + jnp.arange(tok_count)).astype(jnp.float32)
    rotated_q = rotate(queries.reshape(tok_count, q_local, HD), places).reshape(
        blocks, WINDOW, kv_local, group_size, HD
    )
    rotated_k = rotate(key_heads.reshape(tok_count, kv_local, HD), places).reshape(
        tok_count, kv_local * HD
    )
    rimmed = padded(jnp.stack([rotated_k, value_heads]), (("sp", 1),), WINDOW)
    key_win = banded(rimmed[0].reshape(-1, kv_local, HD), blocks)
    val_win = banded(rimmed[1].reshape(-1, kv_local, HD), blocks)
    padded_docs = jnp.pad(doc_ids, (WINDOW, WINDOW), constant_values=-1)
    key_docs = banded(lax.dynamic_slice_in_dim(padded_docs, offset, tok_count + 2 * WINDOW), blocks)
    query_docs = lax.dynamic_slice_in_dim(doc_ids, offset, tok_count).reshape(blocks, WINDOW)
    q_index = jnp.arange(WINDOW)[:, None]
    k_index = jnp.arange(3 * WINDOW)[None, :]
    in_window = jnp.abs(k_index - WINDOW - q_index) <= WINDOW
    allowed = (in_window[None] & (query_docs[:, :, None] == key_docs[:, None, :]))[:, None, None]
    scores = jnp.einsum(
        "nqkgd,nskd->nkgqs", rotated_q, key_win, preferred_element_type=jnp.float32
    ) * HD ** (-0.5)
    masked = jnp.where(allowed, scores, -1e30)
    sink_col = sink_logit.reshape(kv_local, group_size)[None, :, :, None]
    top_score = jnp.maximum(jnp.max(masked, axis=-1), sink_col)
    exp_scores = jnp.where(allowed, jnp.exp(masked - top_score[..., None]), 0.0)
    denom_sum = jnp.sum(exp_scores, axis=-1) + jnp.exp(sink_col - top_score)
    probs = (exp_scores / denom_sum[..., None]).astype(jnp.bfloat16)
    attn = (
        jnp.einsum("nkgqs,nskd->nqkgd", probs, val_win, preferred_element_type=jnp.float32)
        .astype(jnp.bfloat16)
        .reshape(tok_count, q_local * HD)
    )
    partial_mix = jnp.dot(attn, out_proj, preferred_element_type=jnp.float32).astype(jnp.bfloat16)
    mixed = summed_on_arrival(partial_mix, "tp", 0)
    own_resid = lax.dynamic_slice_in_dim(residual, lax.axis_index("tp") * share_rows, share_rows, 0)
    after_mix = (own_resid.astype(jnp.float32) + rms_scale(mixed, gain_mix)).astype(jnp.bfloat16)
    own_normed = rms_scale(after_mix.astype(jnp.float32), gain_ffn_in).astype(jnp.bfloat16)
    normed = exchanged(jnp.broadcast_to(own_normed[None], (8, *own_normed.shape)))
    normed = normed.reshape(-1, 2048)
    other_normed = swapped(normed)
    other_hidden = lax.optimization_barrier(ffn_up(other_normed, weights))
    other_part = ffn_down(other_hidden, weights).astype(jnp.bfloat16)
    received = swapped(other_part)
    hidden = lax.optimization_barrier(ffn_up(normed, weights))
    own_part = lax.optimization_barrier(ffn_down(hidden, weights))
    both_parts = (own_part + received.astype(jnp.float32)).astype(jnp.bfloat16)
    ffn_out = exchanged(both_parts.reshape(8, -1, 2048)).astype(jnp.float32).sum(axis=0)
    return (after_mix.astype(jnp.float32) + rms_scale(ffn_out, gain_ffn_out)).astype(jnp.bfloat16)


def solution(mesh):
    return jax.shard_map(
        body,
        mesh=mesh,
        in_specs=(
            P("sp", "tp"),
            P("sp", "tp"),
            P("sp", "tp"),
            P("tp"),
            P(),
            P("sp", None),
            P("tp", None),
            P(),
            P("sp", "tp"),
            P("tp", "sp"),
            P(),
            P(),
        ),
        out_specs=P(("sp", "tp"), None),
        check_vma=False,
    )
```

```python
import jax
import jax.numpy as jnp
from jax import lax
from jax.sharding import PartitionSpec as P

HD = 128
WINDOW = 128


def device(z, y, x, core):
    return (4 * z + y) * 8 + 2 * x + core


def swapped(shard):
    return lax.ppermute(shard, "tp", [(i, i ^ 1) for i in range(8)])


def token_groups():
    return [
        [device(z, 2 * q + par, x, core) for par in range(2) for x in range(4)]
        for z in range(16)
        for q in range(2)
        for core in range(2)
    ]


def exchanged(pieces):
    return lax.all_to_all(
        pieces, ("sp", "tp"), 0, 0, axis_index_groups=token_groups(), tiled=True
    )


def group_weights(up_proj, down_proj):
    down_rows = down_proj.T
    pieces = jnp.concatenate(
        [jnp.stack([w[:, :512], w[:, 512:]] * 2) for w in (up_proj, down_rows)], axis=2
    )
    along_y = [[4 * z + y for y in range(4)] for z in range(16)]
    along_z = [[4 * z + y for z in range(16)] for y in range(4)]
    rows = lax.all_to_all(
        pieces, "sp", 0, 0, axis_index_groups=along_y, tiled=True
    )
    return lax.all_gather(
        rows.reshape(128, 1024), "sp", axis=0, tiled=True, axis_index_groups=along_z
    )


def ffn_up(normed, both):
    up_acts = jnp.dot(normed, both, preferred_element_type=jnp.float32)
    return jnp.square(jax.nn.relu(up_acts)).astype(jnp.bfloat16)


def ffn_down(hidden, both):
    across = (((1,), (1,)), ((), ()))
    return lax.dot_general(hidden, both[:, 512:], across, preferred_element_type=jnp.float32)


def padded(shard, sides, width):
    for axis, dim in sides:
        devices, length = (lax.axis_size(axis), shard.shape[dim])
        up = [(i, (i + 1) % devices) for i in range(devices - 1)]
        down = [(j, i) for i, j in up]
        last = lax.slice_in_dim(shard, length - width, length, axis=dim)
        first = lax.slice_in_dim(shard, 0, width, axis=dim)
        before = lax.ppermute(last, axis, up)
        after = lax.ppermute(first, axis, down)
        shard = jnp.concatenate([before, shard, after], axis=dim)
    return shard


def split_up(shard, dim, devices):
    before, after = (shard.shape[:dim], shard.shape[dim + 1 :])
    return jnp.moveaxis(shard.reshape(*before, devices, -1, *after), dim, 0)


def summed_on_arrival(shard, axis, dim):
    pieces = split_up(shard, dim, lax.axis_size(axis))
    arrived = lax.all_to_all(pieces, axis, split_axis=0, concat_axis=0, tiled=True)
    return arrived.astype(jnp.float32).sum(axis=0)


def rotate(field, places):
    half_dim = HD // 2
    inv_freq = 10000.0 ** (-jnp.arange(0, HD, 2, dtype=jnp.float32) / HD)
    angles = places[:, None, None] * inv_freq[None, None, :]
    cosine = jnp.cos(angles)
    sine = jnp.sin(angles)
    lower = field[..., :half_dim].astype(jnp.float32)
    upper = field[..., half_dim:].astype(jnp.float32)
    return jnp.concatenate(
        [lower * cosine - upper * sine, upper * cosine + lower * sine], axis=-1
    ).astype(jnp.bfloat16)


def banded(field, blocks):
    framed = field.reshape((blocks + 2, WINDOW) + field.shape[1:])
    return jnp.concatenate([framed[:-2], framed[1:-1], framed[2:]], axis=1)


def rms_scale(field, gain_vec):
    return field * lax.rsqrt(jnp.mean(field * field, axis=-1, keepdims=True) + 1e-06) * gain_vec


def body(
    queries,
    key_heads,
    value_heads,
    sink_logit,
    doc_ids,
    residual,
    out_proj,
    gain_mix,
    up_proj,
    down_proj,
    gain_ffn_in,
    gain_ffn_out,
):
    tok_count = queries.shape[0]
    blocks = tok_count // WINDOW
    share_rows = tok_count // lax.axis_size("tp")
    q_local = queries.shape[1] // HD
    kv_local = key_heads.shape[1] // HD
    group_size = q_local // kv_local
    offset = lax.axis_index("sp") * tok_count
    weights = group_weights(up_proj, down_proj)
    places = (offset + jnp.arange(tok_count)).astype(jnp.float32)
    rotated_q = rotate(queries.reshape(tok_count, q_local, HD), places).reshape(
        blocks, WINDOW, kv_local, group_size, HD
    )
    rotated_k = rotate(key_heads.reshape(tok_count, kv_local, HD), places).reshape(
        tok_count, kv_local * HD
    )
    rimmed = padded(jnp.stack([rotated_k, value_heads]), (("sp", 1),), WINDOW)
    key_win = banded(rimmed[0].reshape(-1, kv_local, HD), blocks)
    val_win = banded(rimmed[1].reshape(-1, kv_local, HD), blocks)
    padded_docs = jnp.pad(doc_ids, (WINDOW, WINDOW), constant_values=-1)
    key_docs = banded(lax.dynamic_slice_in_dim(padded_docs, offset, tok_count + 2 * WINDOW), blocks)
    query_docs = lax.dynamic_slice_in_dim(doc_ids, offset, tok_count).reshape(blocks, WINDOW)
    q_index = jnp.arange(WINDOW)[:, None]
    k_index = jnp.arange(3 * WINDOW)[None, :]
    in_window = jnp.abs(k_index - WINDOW - q_index) <= WINDOW
    allowed = (in_window[None] & (query_docs[:, :, None] == key_docs[:, None, :]))[:, None, None]
    scores = jnp.einsum(
        "nqkgd,nskd->nkgqs", rotated_q, key_win, preferred_element_type=jnp.float32
    ) * HD ** (-0.5)
    masked = jnp.where(allowed, scores, -1e30)
    sink_col = sink_logit.reshape(kv_local, group_size)[None, :, :, None]
    top_score = jnp.maximum(jnp.max(masked, axis=-1), sink_col)
    exp_scores = jnp.where(allowed, jnp.exp(masked - top_score[..., None]), 0.0)
    denom_sum = jnp.sum(exp_scores, axis=-1) + jnp.exp(sink_col - top_score)
    probs = (exp_scores / denom_sum[..., None]).astype(jnp.bfloat16)
    attn = (
        jnp.einsum("nkgqs,nskd->nqkgd", probs, val_win, preferred_element_type=jnp.float32)
        .astype(jnp.bfloat16)
        .reshape(tok_count, q_local * HD)
    )
    partial_mix = jnp.dot(attn, out_proj, preferred_element_type=jnp.float32).astype(jnp.bfloat16)
    mixed = summed_on_arrival(partial_mix, "tp", 0)
    own_resid = lax.dynamic_slice_in_dim(residual, lax.axis_index("tp") * share_rows, share_rows, 0)
    after_mix = (own_resid.astype(jnp.float32) + rms_scale(mixed, gain_mix)).astype(jnp.bfloat16)
    own_normed = rms_scale(after_mix.astype(jnp.float32), gain_ffn_in).astype(jnp.bfloat16)
    normed = exchanged(jnp.broadcast_to(own_normed[None], (8, *own_normed.shape)))
    normed = normed.reshape(-1, 2048)
    other_normed = swapped(normed)
    first = lax.optimization_barrier(ffn_up(other_normed, weights[:, :256]))
    second = lax.optimization_barrier(ffn_up(other_normed, weights[:, 256:512]))
    other_hidden = jnp.concatenate([first, second], axis=1)
    other_part = ffn_down(other_hidden, weights).astype(jnp.bfloat16)
    received = swapped(other_part)
    hidden = lax.optimization_barrier(ffn_up(normed, weights[:, :512]))
    own_part = lax.optimization_barrier(ffn_down(hidden, weights))
    both_parts = (own_part + received.astype(jnp.float32)).astype(jnp.bfloat16)
    ffn_out = exchanged(both_parts.reshape(8, -1, 2048)).astype(jnp.float32).sum(axis=0)
    return (after_mix.astype(jnp.float32) + rms_scale(ffn_out, gain_ffn_out)).astype(jnp.bfloat16)


def solution(mesh):
    return jax.shard_map(
        body,
        mesh=mesh,
        in_specs=(
            P("sp", "tp"),
            P("sp", "tp"),
            P("sp", "tp"),
            P("tp"),
            P(),
            P("sp", None),
            P("tp", None),
            P(),
            P("sp", "tp"),
            P("tp", "sp"),
            P(),
            P(),
        ),
        out_specs=P(("sp", "tp"), None),
        check_vma=False,
    )
```

```python
import jax
import jax.numpy as jnp
from jax import lax
from jax.sharding import PartitionSpec as P

HD = 128
WINDOW = 128


def device(z, y, x, core):
    return (4 * z + y) * 8 + 2 * x + core


def swapped(shard):
    return lax.ppermute(shard, "tp", [(i, i ^ 1) for i in range(8)])


def token_groups():
    return [
        [device(z, 2 * q + par, x, core) for par in range(2) for x in range(4)]
        for z in range(16)
        for q in range(2)
        for core in range(2)
    ]


def exchanged(pieces):
    return lax.all_to_all(
        pieces, ("sp", "tp"), 0, 0, axis_index_groups=token_groups(), tiled=True
    )


def group_weights(up_proj, down_proj):
    down_rows = down_proj.T
    pieces = jnp.concatenate(
        [jnp.stack([w[:, :512], w[:, 512:]] * 2) for w in (up_proj, down_rows)], axis=2
    )
    along_y = [[4 * z + y for y in range(4)] for z in range(16)]
    along_z = [[4 * z + y for z in range(16)] for y in range(4)]
    rows = lax.all_to_all(
        pieces, "sp", 0, 0, axis_index_groups=along_y, tiled=True
    )
    return lax.all_gather(
        rows.reshape(128, 1024), "sp", axis=0, tiled=True, axis_index_groups=along_z
    )


def ffn_up(normed, both):
    up_acts = jnp.dot(normed, both[:, :512], preferred_element_type=jnp.float32)
    return jnp.square(jax.nn.relu(up_acts)).astype(jnp.bfloat16)


def ffn_down(hidden, both):
    across = (((1,), (1,)), ((), ()))
    return lax.dot_general(hidden, both[:, 512:], across, preferred_element_type=jnp.float32)


def padded(shard, sides, width):
    for axis, dim in sides:
        devices, length = (lax.axis_size(axis), shard.shape[dim])
        up = [(i, (i + 1) % devices) for i in range(devices - 1)]
        down = [(j, i) for i, j in up]
        last = lax.slice_in_dim(shard, length - width, length, axis=dim)
        first = lax.slice_in_dim(shard, 0, width, axis=dim)
        before = lax.ppermute(last, axis, up)
        after = lax.ppermute(first, axis, down)
        shard = jnp.concatenate([before, shard, after], axis=dim)
    return shard


def split_up(shard, dim, devices):
    before, after = (shard.shape[:dim], shard.shape[dim + 1 :])
    return jnp.moveaxis(shard.reshape(*before, devices, -1, *after), dim, 0)


def summed_on_arrival(shard, axis, dim):
    pieces = split_up(shard, dim, lax.axis_size(axis))
    arrived = lax.all_to_all(pieces, axis, split_axis=0, concat_axis=0, tiled=True)
    return arrived.astype(jnp.float32).sum(axis=0)


def rotate(field, places):
    half_dim = HD // 2
    inv_freq = 10000.0 ** (-jnp.arange(0, HD, 2, dtype=jnp.float32) / HD)
    angles = places[:, None, None] * inv_freq[None, None, :]
    cosine = jnp.cos(angles)
    sine = jnp.sin(angles)
    lower = field[..., :half_dim].astype(jnp.float32)
    upper = field[..., half_dim:].astype(jnp.float32)
    return jnp.concatenate(
        [lower * cosine - upper * sine, upper * cosine + lower * sine], axis=-1
    ).astype(jnp.bfloat16)


def banded(field, blocks):
    framed = field.reshape((blocks + 2, WINDOW) + field.shape[1:])
    return jnp.concatenate([framed[:-2], framed[1:-1], framed[2:]], axis=1)


def rms_scale(field, gain_vec):
    return field * lax.rsqrt(jnp.mean(field * field, axis=-1, keepdims=True) + 1e-06) * gain_vec


def body(
    queries,
    key_heads,
    value_heads,
    sink_logit,
    doc_ids,
    residual,
    out_proj,
    gain_mix,
    up_proj,
    down_proj,
    gain_ffn_in,
    gain_ffn_out,
):
    tok_count = queries.shape[0]
    blocks = tok_count // WINDOW
    share_rows = tok_count // lax.axis_size("tp")
    q_local = queries.shape[1] // HD
    kv_local = key_heads.shape[1] // HD
    group_size = q_local // kv_local
    offset = lax.axis_index("sp") * tok_count
    weights = group_weights(up_proj, down_proj)
    places = (offset + jnp.arange(tok_count)).astype(jnp.float32)
    rotated_q = rotate(queries.reshape(tok_count, q_local, HD), places).reshape(
        blocks, WINDOW, kv_local, group_size, HD
    )
    rotated_k = rotate(key_heads.reshape(tok_count, kv_local, HD), places).reshape(
        tok_count, kv_local * HD
    )
    rimmed = padded(jnp.stack([rotated_k, value_heads]), (("sp", 1),), WINDOW)
    key_win = banded(rimmed[0].reshape(-1, kv_local, HD), blocks)
    val_win = banded(rimmed[1].reshape(-1, kv_local, HD), blocks)
    padded_docs = jnp.pad(doc_ids, (WINDOW, WINDOW), constant_values=-1)
    key_docs = banded(lax.dynamic_slice_in_dim(padded_docs, offset, tok_count + 2 * WINDOW), blocks)
    query_docs = lax.dynamic_slice_in_dim(doc_ids, offset, tok_count).reshape(blocks, WINDOW)
    q_index = jnp.arange(WINDOW)[:, None]
    k_index = jnp.arange(3 * WINDOW)[None, :]
    in_window = jnp.abs(k_index - WINDOW - q_index) <= WINDOW
    allowed = (in_window[None] & (query_docs[:, :, None] == key_docs[:, None, :]))[:, None, None]
    scores = jnp.einsum(
        "nqkgd,nskd->nkgqs", rotated_q, key_win, preferred_element_type=jnp.float32
    ) * HD ** (-0.5)
    masked = jnp.where(allowed, scores, -1e30)
    sink_col = sink_logit.reshape(kv_local, group_size)[None, :, :, None]
    top_score = jnp.maximum(jnp.max(masked, axis=-1), sink_col)
    exp_scores = jnp.where(allowed, jnp.exp(masked - top_score[..., None]), 0.0)
    denom_sum = jnp.sum(exp_scores, axis=-1) + jnp.exp(sink_col - top_score)
    probs = (exp_scores / denom_sum[..., None]).astype(jnp.bfloat16)
    attn = (
        jnp.einsum("nkgqs,nskd->nqkgd", probs, val_win, preferred_element_type=jnp.float32)
        .astype(jnp.bfloat16)
        .reshape(tok_count, q_local * HD)
    )
    partial_mix = jnp.dot(attn, out_proj, preferred_element_type=jnp.float32).astype(jnp.bfloat16)
    mixed = summed_on_arrival(partial_mix, "tp", 0)
    own_resid = lax.dynamic_slice_in_dim(residual, lax.axis_index("tp") * share_rows, share_rows, 0)
    after_mix = (own_resid.astype(jnp.float32) + rms_scale(mixed, gain_mix)).astype(jnp.bfloat16)
    own_normed = rms_scale(after_mix.astype(jnp.float32), gain_ffn_in).astype(jnp.bfloat16)
    normed = exchanged(jnp.broadcast_to(own_normed[None], (8, *own_normed.shape)))
    normed = normed.reshape(-1, 2048)
    other_normed = swapped(normed)
    other_hidden = lax.optimization_barrier(ffn_up(other_normed, weights))
    other_part = ffn_down(other_hidden, weights).astype(jnp.bfloat16)
    received = swapped(other_part)
    hidden = lax.optimization_barrier(ffn_up(normed, weights))
    own_part = lax.optimization_barrier(ffn_down(hidden, weights).astype(jnp.bfloat16))
    both_parts = (own_part.astype(jnp.float32) + received.astype(jnp.float32)).astype(jnp.bfloat16)
    ffn_out = exchanged(both_parts.reshape(8, -1, 2048)).astype(jnp.float32).sum(axis=0)
    return (after_mix.astype(jnp.float32) + rms_scale(ffn_out, gain_ffn_out)).astype(jnp.bfloat16)


def solution(mesh):
    return jax.shard_map(
        body,
        mesh=mesh,
        in_specs=(
            P("sp", "tp"),
            P("sp", "tp"),
            P("sp", "tp"),
            P("tp"),
            P(),
            P("sp", None),
            P("tp", None),
            P(),
            P("sp", "tp"),
            P("tp", "sp"),
            P(),
            P(),
        ),
        out_specs=P(("sp", "tp"), None),
        check_vma=False,
    )
```

```python
import jax
import jax.numpy as jnp
from jax import lax
from jax.sharding import PartitionSpec as P

HD = 128
WINDOW = 128


def device(z, y, x, core):
    return (4 * z + y) * 8 + 2 * x + core


def swapped(shard):
    return lax.ppermute(shard, "tp", [(i, i ^ 1) for i in range(8)])


def token_groups():
    return [
        [device(z, 2 * q + par, x, core) for par in range(2) for x in range(4)]
        for z in range(16)
        for q in range(2)
        for core in range(2)
    ]


def exchanged(pieces):
    return lax.all_to_all(
        pieces, ("sp", "tp"), 0, 0, axis_index_groups=token_groups(), tiled=True
    )


def group_weights(up_proj, down_proj):
    down_rows = down_proj.T
    pieces = jnp.concatenate(
        [jnp.stack([w[:, :512], w[:, 512:]] * 2) for w in (up_proj, down_rows)], axis=2
    )
    along_y = [[4 * z + y for y in range(4)] for z in range(16)]
    along_z = [[4 * z + y for z in range(16)] for y in range(4)]
    rows = lax.all_to_all(
        pieces, "sp", 0, 0, axis_index_groups=along_y, tiled=True
    )
    return lax.all_gather(
        rows.reshape(128, 1024), "sp", axis=0, tiled=True, axis_index_groups=along_z
    )


def ffn_up(normed, both):
    up_acts = jnp.dot(normed, both[:, :512], preferred_element_type=jnp.float32)
    return jnp.square(jax.nn.relu(up_acts)).astype(jnp.bfloat16)


def ffn_down(hidden, both):
    across = (((1,), (1,)), ((), ()))
    return lax.dot_general(hidden, both[:, 512:], across, preferred_element_type=jnp.float32)


def padded(shard, sides, width):
    for axis, dim in sides:
        devices, length = (lax.axis_size(axis), shard.shape[dim])
        up = [(i, (i + 1) % devices) for i in range(devices - 1)]
        down = [(j, i) for i, j in up]
        last = lax.slice_in_dim(shard, length - width, length, axis=dim)
        first = lax.slice_in_dim(shard, 0, width, axis=dim)
        before = lax.ppermute(last, axis, up)
        after = lax.ppermute(first, axis, down)
        shard = jnp.concatenate([before, shard, after], axis=dim)
    return shard


def split_up(shard, dim, devices):
    before, after = (shard.shape[:dim], shard.shape[dim + 1 :])
    return jnp.moveaxis(shard.reshape(*before, devices, -1, *after), dim, 0)


def summed_on_arrival(shard, axis, dim):
    pieces = split_up(shard, dim, lax.axis_size(axis))
    arrived = lax.all_to_all(pieces, axis, split_axis=0, concat_axis=0, tiled=True)
    return arrived.astype(jnp.float32).sum(axis=0)


def rotate(field, places):
    half_dim = HD // 2
    inv_freq = 10000.0 ** (-jnp.arange(0, HD, 2, dtype=jnp.float32) / HD)
    angles = places[:, None, None] * inv_freq[None, None, :]
    cosine = jnp.cos(angles)
    sine = jnp.sin(angles)
    lower = field[..., :half_dim].astype(jnp.float32)
    upper = field[..., half_dim:].astype(jnp.float32)
    return jnp.concatenate(
        [lower * cosine - upper * sine, upper * cosine + lower * sine], axis=-1
    ).astype(jnp.bfloat16)


def banded(field, blocks):
    framed = field.reshape((blocks + 2, WINDOW) + field.shape[1:])
    return jnp.concatenate([framed[:-2], framed[1:-1], framed[2:]], axis=1)


def rms_scale(field, gain_vec):
    return field * lax.rsqrt(jnp.mean(field * field, axis=-1, keepdims=True) + 1e-06) * gain_vec


def body(
    queries,
    key_heads,
    value_heads,
    sink_logit,
    doc_ids,
    residual,
    out_proj,
    gain_mix,
    up_proj,
    down_proj,
    gain_ffn_in,
    gain_ffn_out,
):
    tok_count = queries.shape[0]
    blocks = tok_count // WINDOW
    share_rows = tok_count // lax.axis_size("tp")
    q_local = queries.shape[1] // HD
    kv_local = key_heads.shape[1] // HD
    group_size = q_local // kv_local
    offset = lax.axis_index("sp") * tok_count
    weights = group_weights(up_proj, down_proj)
    places = (offset + jnp.arange(tok_count)).astype(jnp.float32)
    rotated_q = rotate(queries.reshape(tok_count, q_local, HD), places).reshape(
        blocks, WINDOW, kv_local, group_size, HD
    )
    rotated_k = rotate(key_heads.reshape(tok_count, kv_local, HD), places).reshape(
        tok_count, kv_local * HD
    )
    rimmed = padded(jnp.stack([rotated_k, value_heads]), (("sp", 1),), WINDOW)
    key_win = banded(rimmed[0].reshape(-1, kv_local, HD), blocks)
    val_win = banded(rimmed[1].reshape(-1, kv_local, HD), blocks)
    padded_docs = jnp.pad(doc_ids, (WINDOW, WINDOW), constant_values=-1)
    key_docs = banded(lax.dynamic_slice_in_dim(padded_docs, offset, tok_count + 2 * WINDOW), blocks)
    query_docs = lax.dynamic_slice_in_dim(doc_ids, offset, tok_count).reshape(blocks, WINDOW)
    q_index = jnp.arange(WINDOW)[:, None]
    k_index = jnp.arange(3 * WINDOW)[None, :]
    in_window = jnp.abs(k_index - WINDOW - q_index) <= WINDOW
    allowed = (in_window[None] & (query_docs[:, :, None] == key_docs[:, None, :]))[:, None, None]
    scores = jnp.einsum(
        "nqkgd,nskd->nkgqs", rotated_q, key_win, preferred_element_type=jnp.float32
    ) * HD ** (-0.5)
    masked = jnp.where(allowed, scores, -1e30)
    sink_col = sink_logit.reshape(kv_local, group_size)[None, :, :, None]
    top_score = jnp.maximum(jnp.max(masked, axis=-1), sink_col)
    exp_scores = jnp.where(allowed, jnp.exp(masked - top_score[..., None]), 0.0)
    denom_sum = jnp.sum(exp_scores, axis=-1) + jnp.exp(sink_col - top_score)
    probs = (exp_scores / denom_sum[..., None]).astype(jnp.bfloat16)
    attn = (
        jnp.einsum("nkgqs,nskd->nqkgd", probs, val_win, preferred_element_type=jnp.float32)
        .astype(jnp.bfloat16)
        .reshape(tok_count, q_local * HD)
    )
    partial_mix = jnp.dot(attn, out_proj, preferred_element_type=jnp.float32).astype(jnp.bfloat16)
    mixed = summed_on_arrival(partial_mix, "tp", 0)
    own_resid = lax.dynamic_slice_in_dim(residual, lax.axis_index("tp") * share_rows, share_rows, 0)
    after_mix = (own_resid.astype(jnp.float32) + rms_scale(mixed, gain_mix)).astype(jnp.bfloat16)
    own_normed = rms_scale(after_mix.astype(jnp.float32), gain_ffn_in).astype(jnp.bfloat16)
    normed = exchanged(jnp.broadcast_to(own_normed[None], (8, *own_normed.shape)))
    normed = normed.reshape(-1, 2048)
    other_normed = [swapped(normed[:, :1024]), swapped(normed[:, 1024:])]
    other_hidden = lax.optimization_barrier(ffn_up(jnp.concatenate(other_normed, axis=1), weights))
    other_part = ffn_down(other_hidden, weights).astype(jnp.bfloat16)
    received = swapped(other_part)
    hidden = lax.optimization_barrier(ffn_up(normed, weights))
    own_part = lax.optimization_barrier(ffn_down(hidden, weights))
    both_parts = (own_part + received.astype(jnp.float32)).astype(jnp.bfloat16)
    ffn_out = exchanged(both_parts.reshape(8, -1, 2048)).astype(jnp.float32).sum(axis=0)
    return (after_mix.astype(jnp.float32) + rms_scale(ffn_out, gain_ffn_out)).astype(jnp.bfloat16)


def solution(mesh):
    return jax.shard_map(
        body,
        mesh=mesh,
        in_specs=(
            P("sp", "tp"),
            P("sp", "tp"),
            P("sp", "tp"),
            P("tp"),
            P(),
            P("sp", None),
            P("tp", None),
            P(),
            P("sp", "tp"),
            P("tp", "sp"),
            P(),
            P(),
        ),
        out_specs=P(("sp", "tp"), None),
        check_vma=False,
    )
```
